256 devices in a mesh: sp: 64 (over z, y, core), tp: 4 (over x).
Axes of the slice: x: 4, y: 4, z: 8, core: 2. Of those that a mesh axis runs over, the one named last changes fastest.
Arguments:
- stream: bfloat16 [8192, 2048], P('sp'), may hold values from -12 to 12
- out_grad: bfloat16 [8192, 2048], P('sp'), may hold values from -16 to 16
- routes: int32 [8192, 2], P('sp'), may hold values from 0 to 63, all different within a row; in each aligned block of 128 rows (0 to 127, 128 to 255, ...) at most 8 rows name the same one
- route_weight: float32 [8192, 2], P('sp'), may hold values from 0.2 to 1
- queries: bfloat16 [8192, 8, 128], P('sp', 'tp'), may hold values from -6 to 6
- key_vectors: bfloat16 [8192, 8, 128], P('sp', 'tp'), may hold values from -6 to 6
- value_vectors: bfloat16 [8192, 8, 256], P('sp', 'tp'), may hold values from -6 to 6
- log_decay: float32 [8192, 8], P('sp', 'tp'), may hold values from -1 to 0
- out_proj: bfloat16 [2048, 2048], P(None, 'tp'), may hold values from -0.125 to 0.125
- gate_weight: bfloat16 [64, 2048, 1024], P('sp', None, 'tp'), may hold values from -0.125 to 0.125
- up_weight: bfloat16 [64, 2048, 1024], P('sp', None, 'tp'), may hold values from -0.125 to 0.125
- down_weight: bfloat16 [64, 1024, 2048], P('sp', 'tp'), may hold values from -0.1875 to 0.1875
Outputs:
- gate_grad: bfloat16 [64, 2048, 1024], P('sp', None, 'tp')
- up_grad: bfloat16 [64, 2048, 1024], P('sp', None, 'tp')
- down_grad: bfloat16 [64, 1024, 2048], P('sp', 'tp')
- proj_grad: float32 [2048, 2048], P('sp', 'tp')
- query_grad: bfloat16 [8192, 8, 128], P('sp', 'tp')
- key_grad: bfloat16 [8192, 8, 128], P('sp', 'tp')
- value_grad: bfloat16 [8192, 8, 256], P('sp', 'tp')
The draws below stay inside these ranges and needn't reach their ends.
Inputs may be any that keep to these rules, and one draw needn't show every extreme that they name: `routes`: each row names two different experts. In each aligned block of 128 rows no expert is named by more than 8 rows, and in some block an expert is named by exactly 8.
All inputs are finite; a program needn't handle non-finite values.
Results may differ from the reference program's by a relative error of at most 0.025.
Values may be sent and summed in bfloat16 or wider, within the bound.
A program may use at most 128 MiB of HBM per device.

```python
import math
import jax
import jax.numpy as jnp
import numpy as np
from jax import lax

D = 2048
RETENTION_HEADS = 8
KD = 128
VD = 256
FF = 1024
TOK_DEV = 128
SEQUENCE_TOKENS = 8192
EXPERTS = 64
CAP = 8
HV = 2048
N_SP = 64
N_TP = 4


def draw_log_decay(key, part):
    random_subkeys = jax.random.split(jax.random.fold_in(key, 7), 7)
    ranking = jax.random.permutation(random_subkeys[0], RETENTION_HEADS)
    slow_rate = jax.random.uniform(random_subkeys[1], (RETENTION_HEADS,), jnp.float32, 0.05, 0.2) / SEQUENCE_TOKENS
    fast_rate = jnp.exp(jax.random.uniform(random_subkeys[2], (RETENTION_HEADS,), jnp.float32, math.log(0.012), math.log(0.025)))
    baseline_decay_rate = jnp.where(ranking < RETENTION_HEADS // 2, fast_rate, slow_rate)
    decay_factor = jnp.exp(jax.random.uniform(random_subkeys[3], (SEQUENCE_TOKENS // TOK_DEV, RETENTION_HEADS), jnp.float32, 0.0, math.log(3.0)))
    decay_factor = jnp.repeat(decay_factor, TOK_DEV, axis=0)
    jitter_amount = jax.random.uniform(random_subkeys[4], (SEQUENCE_TOKENS, RETENTION_HEADS), jnp.float32, 0.6, 1.4)
    spike_location = jax.random.randint(random_subkeys[5], (2, RETENTION_HEADS), 0, SEQUENCE_TOKENS)
    spike_depth = jax.random.uniform(random_subkeys[6], (2, RETENTION_HEADS), jnp.float32, math.log(0.5), math.log(0.8))
    token_position = jnp.arange(SEQUENCE_TOKENS, dtype=jnp.int32)[:, None]
    spike_events = jnp.where(token_position == spike_location[0][None, :], spike_depth[0][None, :], 0.0)
    spike_events = spike_events + jnp.where(token_position == spike_location[1][None, :], spike_depth[1][None, :], 0.0)
    return -(baseline_decay_rate[None, :] * decay_factor * jitter_amount) + spike_events


def strengthened(drawn, own_key, source, target, shards_of, factor):
    def block_of(position):
        return (jnp.arange(drawn.shape[position]) // (drawn.shape[position] // shards_of)).reshape((-1,) + (1,) * (drawn.ndim - 1 - position))

    first = jax.random.permutation(own_key, shards_of)[block_of(target)]
    far = (block_of(target) + shards_of // 2) % shards_of
    return jnp.where((block_of(source) == first) | (block_of(source) == far), factor * drawn, drawn)


def block_levels(rng, extent, cuts, least, largest):
    loudness, own = 1.0, jax.random.fold_in(rng, 6)
    for position, blocks in cuts:
        draws = jnp.exp(jax.random.uniform(jax.random.fold_in(own, position), (blocks,), jnp.float32, least / len(cuts), largest / len(cuts)))
        loudness = loudness * jnp.repeat(draws, extent[position] // blocks).reshape([-1 if axis == position else 1 for axis in range(len(extent))])
    return loudness


def deal_out(own_key, own, number, rows, count, top, reach, skew):
    sequence = jax.random.permutation(own_key, count)
    heavy_load, common = portions_of(count, rows * top, reach, skew, True), portions_of(count, rows * top, reach, skew, False)
    places = jnp.arange(count)

    def named(sizes, rotation):
        used = int((sizes > 0).sum())
        fixed = max(1, used // 4)
        moved = fixed + (places - fixed + rotation * (used - fixed)) % max(1, count - fixed)
        return jnp.zeros((count,), jnp.int32).at[sequence[jnp.where(places < fixed, places, moved)]].set(jnp.asarray(sizes, jnp.int32))

    sizes = jnp.where(number % 4 == 0, named(heavy_load, number // 4), named(common, number - number // 4 - 1))
    mixed = jax.random.permutation(jax.random.fold_in(own, 3), count)
    donor, taker = mixed[0:count // 2 * 2:2], mixed[1:count // 2 * 2:2]
    slack = jnp.minimum(sizes[donor] - 1, reach - sizes[taker]) // 2
    slack = jnp.where((donor == sequence[0]) | (taker == sequence[0]) | (sizes[taker] == 0), 0, jnp.maximum(slack, 0))
    moved = jax.random.randint(jax.random.fold_in(own, 4), (count // 2,), 0, 1 << 20) % (slack + 1)
    sizes = sizes.at[donor].add(-moved).at[taker].add(moved)
    members = jnp.searchsorted(jnp.cumsum(sizes), jnp.arange(rows * top), side="right").astype(jnp.int32)
    listing = members.reshape(top, rows).T
    listing = listing[jax.random.permutation(jax.random.fold_in(own, 1), rows)]
    rotation = jax.random.randint(jax.random.fold_in(own, 2), (rows, 1), 0, top)
    return jnp.take_along_axis(listing, (jnp.arange(top)[None, :] + rotation) % top, axis=1)


def portions_of(number_of, total, most, skew, full):
    loads = [(1 << 20) // math.isqrt(standing ** skew) + 1 for standing in range(1, number_of + 1)]
    largest = most if full else min(most, max(-(-total // number_of), total * loads[0] // sum(loads)))
    least = 1 if total - largest >= number_of - 1 else 0
    given, spare = [largest] + [least] * (number_of - 1), total - largest - least * (number_of - 1)
    while spare > 0:
        movable = [i for i in range(1, number_of) if given[i] < largest] or [i for i in range(1, number_of) if given[i] < most]
        pool, remaining = sum([loads[i] for i in movable]), spare
        for i in movable:
            more = min(most - given[i], max(1, remaining * loads[i] // pool), spare)
            given[i] = given[i] + more
            spare = spare - more
    return np.array(given)


def bell_draw(own_key, extent, scale, limit, cuts=(), kind=jnp.bfloat16):
    level = block_levels(own_key, extent, cuts, -0.22, 0.18) if cuts else 1.0
    values = jax.random.normal(own_key, extent, jnp.float32) * scale * level
    return jnp.minimum(jnp.maximum(values, -limit), limit).astype(kind)


def gaussian_with(stream_key, shape, width, limit, cuts, heavy, kind=jnp.bfloat16):
    result = width * jax.random.normal(stream_key, shape, jnp.float32)
    if cuts:
        result = result * block_levels(stream_key, shape, cuts, -0.22, 0.18)
    return jnp.clip(strengthened(result, jax.random.fold_in(stream_key, 3), *heavy), -limit, limit).astype(kind)


def setup_inputs(seed: int = 0) -> dict:
    arg_keys = jax.random.split(jax.random.key(seed), 13)
    stream = bell_draw(arg_keys[0], (SEQUENCE_TOKENS, D), 2.5, 12.0, ((0, 64),))
    out_grad = gaussian_with(arg_keys[1], (SEQUENCE_TOKENS, D), 1.0, 16.0, ((0, 64),), (0, 1, 64, 4.0))
    routes_keys = jax.random.split(jax.random.fold_in(arg_keys[2], 1), SEQUENCE_TOKENS // TOK_DEV)
    routes_turns = jax.random.permutation(jax.random.fold_in(arg_keys[2], 3), SEQUENCE_TOKENS // TOK_DEV)
    routes = jax.vmap(lambda own, number: deal_out(jax.random.fold_in(arg_keys[2], 2), own, number, TOK_DEV, EXPERTS, 2, CAP, 1))(routes_keys, routes_turns).reshape((SEQUENCE_TOKENS, 2))
    route_weight = jnp.clip(jnp.exp(math.log(1.0) - 1.609438 * jax.random.uniform(arg_keys[3], (SEQUENCE_TOKENS, 2), jnp.float32) ** block_levels(arg_keys[3], (SEQUENCE_TOKENS, 2), ((0, 64),), -0.2, 0.2)), 0.2, 1.0)
    queries = bell_draw(arg_keys[4], (SEQUENCE_TOKENS, RETENTION_HEADS, KD), 1.0, 6.0, ((0, 64), (1, 4)))
    key_vectors = bell_draw(arg_keys[5], (SEQUENCE_TOKENS, RETENTION_HEADS, KD), 1.0, 6.0, ((0, 64), (1, 4)))
    value_vectors = bell_draw(arg_keys[6], (SEQUENCE_TOKENS, RETENTION_HEADS, VD), 1.0, 6.0, ((0, 64), (1, 4)))
    log_decay = draw_log_decay(jax.random.fold_in(arg_keys[12], 71), 0)
    out_proj = bell_draw(arg_keys[8], (D, HV), HV ** -0.5, 0.125, ((1, 4),))
    gate_weight = bell_draw(arg_keys[9], (EXPERTS, D, FF), D ** -0.5, 0.125, ((0, 64), (2, 4)))
    up_weight = bell_draw(arg_keys[10], (EXPERTS, D, FF), D ** -0.5, 0.125, ((0, 64), (2, 4)))
    down_weight = bell_draw(arg_keys[11], (EXPERTS, FF, D), FF ** -0.5, 0.1875, ((0, 64), (1, 4)))
    return dict(stream=stream, out_grad=out_grad, routes=routes, route_weight=route_weight, queries=queries, key_vectors=key_vectors, value_vectors=value_vectors, log_decay=log_decay, out_proj=out_proj, gate_weight=gate_weight, up_weight=up_weight, down_weight=down_weight)


CLAMP_LIMIT = 7.0
GATE_SLOPE = 1.702
EPSILON = 1e-06
TOP_PRECISION = lax.Precision.HIGHEST

def slot_numbers(route_block, expert_count):
    flat_ids = route_block.reshape(-1)
    onehot = (flat_ids[:, None] == jnp.arange(expert_count, dtype=jnp.int32)[None, :]).astype(jnp.int32)
    before = jnp.cumsum(onehot, axis=0) - onehot
    return (flat_ids, lax.optimization_barrier(jnp.sum(before * onehot, axis=1)).astype(jnp.int32))

def rotation_tables(start, count, key_width):
    frequency = 1.0 / 10000.0 ** jnp.linspace(0.0, 1.0, key_width // 2, dtype=jnp.float32)
    token_position = (start + jnp.arange(count, dtype=jnp.int32)).astype(jnp.float32)
    angles = token_position[:, None] * frequency[None, :]
    return (jnp.cos(angles), jnp.sin(angles))

def turn(field, cosines, sines):
    paired = field.reshape(field.shape[:-1] + (field.shape[-1] // 2, 2))
    even_part = paired[..., 0]
    odd_part = paired[..., 1]
    cos_rows = cosines[:, None, :]
    sin_rows = sines[:, None, :]
    turned = jnp.stack([even_part * cos_rows - odd_part * sin_rows, odd_part * cos_rows + even_part * sin_rows], axis=-1)
    return turned.reshape(field.shape)

def expert_pass(routed_rows, routed_grads, gate_w, up_w, down_w):
    gate_pre = jnp.dot(routed_rows, gate_w, preferred_element_type=jnp.float32)
    up_pre = jnp.dot(routed_rows, up_w, preferred_element_type=jnp.float32)
    gate_clip = jnp.minimum(gate_pre, CLAMP_LIMIT)
    up_clip = jnp.clip(up_pre, -CLAMP_LIMIT, CLAMP_LIMIT)
    sigmoid_gate = jax.nn.sigmoid(GATE_SLOPE * gate_clip)
    activated = (gate_clip * sigmoid_gate * (up_clip + 1.0)).astype(jnp.bfloat16)
    down_part = lax.dot_general(activated, routed_grads, (((0,), (0,)), ((), ())), preferred_element_type=jnp.float32)
    act_grad = lax.dot_general(routed_grads, down_w, (((1,), (1,)), ((), ())), preferred_element_type=jnp.float32)
    slope = sigmoid_gate + GATE_SLOPE * gate_clip * sigmoid_gate * (1.0 - sigmoid_gate)
    gate_pre_grad = jnp.where(gate_pre < CLAMP_LIMIT, act_grad * (up_clip + 1.0) * slope, 0.0).astype(jnp.bfloat16)
    up_pre_grad = jnp.where(jnp.abs(up_pre) < CLAMP_LIMIT, act_grad * gate_clip * sigmoid_gate, 0.0).astype(jnp.bfloat16)
    gate_part = lax.dot_general(routed_rows, gate_pre_grad, (((0,), (0,)), ((), ())), preferred_element_type=jnp.float32)
    up_part = lax.dot_general(routed_rows, up_pre_grad, (((0,), (0,)), ((), ())), preferred_element_type=jnp.float32)
    row_count = routed_rows.shape[0]
    group = gate_w.shape[1] // N_TP
    gate_groups = gate_pre_grad.reshape(row_count, N_TP, group).astype(jnp.float32)
    up_groups = up_pre_grad.reshape(row_count, N_TP, group).astype(jnp.float32)
    gate_w_groups = gate_w.reshape(gate_w.shape[0], N_TP, group).astype(jnp.float32)
    up_w_groups = up_w.reshape(up_w.shape[0], N_TP, group).astype(jnp.float32)
    partial_value = jnp.einsum('rtf,dtf->trd', gate_groups, gate_w_groups) + jnp.einsum('rtf,dtf->trd', up_groups, up_w_groups)
    rounded = lax.optimization_barrier(partial_value.astype(jnp.bfloat16))
    back_rows = lax.optimization_barrier(jnp.sum(rounded.astype(jnp.float32), axis=0)).astype(jnp.bfloat16)
    return (gate_part.astype(jnp.bfloat16), up_part.astype(jnp.bfloat16), down_part.astype(jnp.bfloat16), back_rows)

def prepare(query_block, key_block, value_block, decay_block, start):
    cosines, sines = rotation_tables(start, TOK_DEV, KD)
    query_rotated = turn(query_block.astype(jnp.float32), cosines, sines).transpose(1, 0, 2)
    key_rotated = (turn(key_block.astype(jnp.float32), cosines, sines) * KD ** (-0.5)).transpose(1, 0, 2)
    value_per_head = value_block.astype(jnp.float32).transpose(1, 0, 2)
    running_total = jnp.cumsum(decay_block, axis=0).T
    block_total = running_total[:, -1]
    causal = (jnp.arange(TOK_DEV)[:, None] >= jnp.arange(TOK_DEV)[None, :])[None]
    difference = running_total[:, :, None] - running_total[:, None, :]
    decay_mask = jnp.where(causal, jnp.exp(jnp.where(causal, difference, 0.0)), 0.0)
    return (query_rotated, key_rotated, value_per_head, running_total, block_total, decay_mask, cosines, sines)

def reference(stream, out_grad, routes, route_weight, queries, key_vectors, value_vectors, log_decay, out_proj, gate_weight, up_weight, down_weight):
    pair_count = 2 * TOK_DEV
    flat_ids, slot_ids = jax.vmap(lambda block_data: slot_numbers(block_data, EXPERTS))(routes.reshape(N_SP, TOK_DEV, 2))
    destination = flat_ids * CAP + slot_ids

    def place(target):
        return jnp.full((EXPERTS * CAP,), -1, jnp.int32).at[target].set(jnp.arange(pair_count, dtype=jnp.int32))
    source = jax.vmap(place)(destination)
    block_ids = jnp.arange(N_SP, dtype=jnp.int32)[:, None]
    present = source >= 0
    global_pair = jnp.where(present, block_ids * pair_count + source, 0).astype(jnp.int32)
    per_expert = global_pair.reshape(N_SP, EXPERTS, CAP).transpose(1, 0, 2).reshape(EXPERTS, N_SP * CAP)
    occupied = present.reshape(N_SP, EXPERTS, CAP).transpose(1, 0, 2).reshape(EXPERTS, N_SP * CAP)
    pair_grad = (route_weight[:, :, None] * out_grad[:, None, :].astype(jnp.float32)).astype(jnp.bfloat16)
    pair_grad = pair_grad.reshape(2 * SEQUENCE_TOKENS, D)
    zero_value = jnp.zeros((), jnp.bfloat16)

    def one_expert(expert_index):
        pair_ids = per_expert[expert_index]
        row_mask = occupied[expert_index][:, None]
        routed_rows = jnp.where(row_mask, jnp.take(stream, pair_ids // 2, axis=0), zero_value)
        routed_grads = jnp.where(row_mask, jnp.take(pair_grad, pair_ids, axis=0), zero_value)
        return expert_pass(routed_rows, routed_grads, gate_weight[expert_index], up_weight[expert_index], down_weight[expert_index])
    gate_grad, up_grad, down_grad, back_rows = lax.map(one_expert, jnp.arange(EXPERTS, dtype=jnp.int32))
    row_index = (flat_ids * (N_SP * CAP) + block_ids * CAP + slot_ids).astype(jnp.int32)
    per_pair = jnp.take(back_rows.reshape(EXPERTS * N_SP * CAP, D), row_index.reshape(-1), axis=0)
    per_pair = per_pair.reshape(SEQUENCE_TOKENS, 2, D).astype(jnp.float32)
    resid_grad = (out_grad.astype(jnp.float32) + per_pair[:, 0] + per_pair[:, 1]).astype(jnp.bfloat16)

    def to_blocks(array):
        return array.reshape((N_SP, TOK_DEV) + array.shape[1:])
    starts = jnp.arange(N_SP, dtype=jnp.int32) * TOK_DEV
    inputs = (to_blocks(queries), to_blocks(key_vectors), to_blocks(value_vectors), to_blocks(log_decay), starts)

    def forward(running_state, block_data):
        query_rotated, key_rotated, value_per_head, running_total, block_total, decay_mask, cosines, sines = prepare(*block_data)
        weights = jnp.einsum('hik,hjk->hij', query_rotated, key_rotated, precision=TOP_PRECISION) * decay_mask
        retained_output = jnp.einsum('hij,hjv->hiv', weights, value_per_head, precision=TOP_PRECISION)
        retained_output = retained_output + jnp.exp(running_total)[..., None] * jnp.einsum('dzr,drs->dzs', query_rotated, running_state, precision=TOP_PRECISION)
        remaining_decay = jnp.exp(block_total[:, None] - running_total)
        inner_state = jnp.einsum('wfs,wfi->wsi', key_rotated * remaining_decay[..., None], value_per_head, precision=TOP_PRECISION)
        new_state = jnp.exp(block_total)[:, None, None] * running_state + inner_state
        return (new_state, (retained_output, running_state))
    _, (retained_all, incoming_state) = lax.scan(forward, jnp.zeros((RETENTION_HEADS, KD, VD), jnp.float32), inputs)
    inverse_rms = lax.rsqrt(lax.optimization_barrier(jnp.mean(retained_all * retained_all, axis=-1, keepdims=True)) + EPSILON)
    normed = retained_all * inverse_rms
    normed_bf = normed.transpose(0, 2, 1, 3).reshape(SEQUENCE_TOKENS, HV).astype(jnp.bfloat16)
    proj_grad = lax.dot_general(resid_grad, normed_bf, (((0,), (0,)), ((), ())), preferred_element_type=jnp.float32)
    normed_grad = jnp.dot(resid_grad, out_proj, preferred_element_type=jnp.float32)
    normed_grad = normed_grad.reshape(N_SP, TOK_DEV, RETENTION_HEADS, VD).transpose(0, 2, 1, 3)
    retention_gradient = inverse_rms * (normed_grad - normed * lax.optimization_barrier(jnp.mean(normed_grad * normed, axis=-1, keepdims=True)))

    def backward(next_rows, block_data):
        block_inputs, running_state, gradient_tile = block_data
        query_rotated, key_rotated, value_per_head, running_total, block_total, decay_mask, cosines, sines = prepare(*block_inputs)
        per_head_decay = jnp.exp(running_total)
        remaining_decay = jnp.exp(block_total[:, None] - running_total)
        weights = jnp.einsum('hik,hjk->hij', query_rotated, key_rotated, precision=TOP_PRECISION) * decay_mask
        score_grad = jnp.einsum('hiv,hjv->hij', gradient_tile, value_per_head, precision=TOP_PRECISION) * decay_mask
        query_portion = jnp.einsum('hij,hjk->hik', score_grad, key_rotated, precision=TOP_PRECISION)
        query_portion = query_portion + per_head_decay[..., None] * jnp.einsum('bpl,btl->bpt', gradient_tile, running_state, precision=TOP_PRECISION)
        key_portion = jnp.einsum('hij,hik->hjk', score_grad, query_rotated, precision=TOP_PRECISION)
        key_portion = key_portion + remaining_decay[..., None] * jnp.einsum('uxn,ubn->uxb', value_per_head, next_rows, precision=TOP_PRECISION)
        value_portion = jnp.einsum('hij,hiv->hjv', weights, gradient_tile, precision=TOP_PRECISION)
        value_portion = value_portion + remaining_decay[..., None] * jnp.einsum('bui,bim->bum', key_rotated, next_rows, precision=TOP_PRECISION)
        inner_gradient = jnp.einsum('gwn,gwj->gnj', query_rotated * per_head_decay[..., None], gradient_tile, precision=TOP_PRECISION)
        earlier_grad = inner_gradient + jnp.exp(block_total)[:, None, None] * next_rows
        q_out = turn(query_portion.transpose(1, 0, 2), cosines, -sines).astype(jnp.bfloat16)
        k_out = (turn(key_portion.transpose(1, 0, 2), cosines, -sines) * KD ** (-0.5)).astype(jnp.bfloat16)
        v_out = value_portion.transpose(1, 0, 2).astype(jnp.bfloat16)
        return (earlier_grad, (q_out, k_out, v_out))
    _, (query_grad, key_grad, value_grad) = lax.scan(backward, jnp.zeros((RETENTION_HEADS, KD, VD), jnp.float32), (inputs, incoming_state, retention_gradient), reverse=True)
    query_grad = query_grad.reshape(SEQUENCE_TOKENS, RETENTION_HEADS, KD)
    key_grad = key_grad.reshape(SEQUENCE_TOKENS, RETENTION_HEADS, KD)
    value_grad = value_grad.reshape(SEQUENCE_TOKENS, RETENTION_HEADS, VD)
    return (gate_grad, up_grad, down_grad, proj_grad, query_grad, key_grad, value_grad)
```

```python
import jax
import jax.numpy as jnp
from jax import lax
from jax.experimental import pallas as pl
from jax.experimental.pallas import tpu as pltpu
from jax.sharding import Mesh
from jax.sharding import PartitionSpec as P

SP = ("sp_0", "sp_1", "sp_2")


CLAMP_LIMIT = 7.0
GATE_SLOPE = 1.702
EPSILON = 1e-06
TOP_PRECISION = lax.Precision.HIGHEST


def in_one_piece(arrays, axis, split_dim, concat_dim, along):
    both = jnp.concatenate(arrays, axis=along)
    result, at, finished = (
        lax.all_to_all(both, axis, split_axis=split_dim, concat_axis=concat_dim, tiled=True),
        0,
        [],
    )
    for a in arrays:
        finished.append(lax.slice_in_dim(result, at, at + a.shape[along], axis=along))
        at += a.shape[along]
    return tuple(finished)


def split_up(x, dim, length):
    before, after = (x.shape[:dim], x.shape[dim + 1 :])
    return jnp.moveaxis(x.reshape(*before, length, -1, *after), dim, 0)


def sent_and_summed(x, axis, dim):
    pieces = split_up(x, dim, lax.axis_size(axis))
    arrived = lax.all_to_all(pieces, axis, split_axis=0, concat_axis=0, tiled=True)
    return arrived.astype(jnp.float32).sum(axis=0)


def copy_for_each(x, axis):
    copies = jnp.broadcast_to(x, (lax.axis_size(axis), *x.shape))
    return lax.all_to_all(copies, axis, split_axis=0, concat_axis=0, tiled=True)


def joined_along(pieces, dim):
    lengths = list(pieces.shape[1:])
    lengths[dim] *= pieces.shape[0]
    return jnp.moveaxis(pieces, 0, dim).reshape(lengths)


def collect(x, axis, dim):
    pieces = copy_for_each(x, axis)
    return joined_along(pieces, dim)


def filled_with(x, identity):
    return jax.tree.map(
        lambda a, e: jnp.broadcast_to(jnp.asarray(e, a.dtype), a.shape), x, identity
    )


def prefix_by_axis(x, axes, combine, identity):
    before = start = filled_with(x, identity)
    total = x
    for axis in reversed(axes):
        length, position = (lax.axis_size(axis), lax.axis_index(axis))
        pieces = jax.tree.map(
            lambda part, kind: lax.all_gather(part.astype(kind), axis),
            total,
            (jnp.bfloat16, jnp.bfloat16),
        )
        inside, total = (start, start)
        for k in range(length):
            passed = k < position
            total = combine(
                total, jax.tree.map(lambda part, own: part[k].astype(own.dtype), pieces, x)
            )
            inside = jax.tree.map(lambda new, old: jnp.where(passed, new, old), total, inside)
        before = combine(inside, before)
    return before


def summed_rows(total, axes):
    for axis in axes:
        total = lax.psum_scatter(total, axis, scatter_dimension=0, tiled=True)
    return total


def prefix_by_axis_2(x, axes, combine, identity):
    before = start = filled_with(x, identity)
    total = x
    for axis in reversed(axes):
        length, position = (lax.axis_size(axis), lax.axis_index(axis))
        pieces = jax.tree.map(
            lambda part, kind: lax.all_gather(part.astype(kind), axis),
            total,
            jax.tree.map(lambda a: jnp.bfloat16 if a.dtype == jnp.float32 else a.dtype, x),
        )
        inside, total = (start, start)
        for k in reversed(range(length)):
            passed = k > position
            total = combine(
                total, jax.tree.map(lambda part, own: part[k].astype(own.dtype), pieces, x)
            )
            inside = jax.tree.map(lambda new, old: jnp.where(passed, new, old), total, inside)
        before = combine(inside, before)
    return before


def slot_numbers(route_block, expert_count):
    flat_ids = route_block.reshape(-1)
    onehot = (flat_ids[:, None] == jnp.arange(expert_count, dtype=jnp.int32)[None, :]).astype(
        jnp.int32
    )
    before = jnp.cumsum(onehot, axis=0) - onehot
    return (flat_ids, jnp.sum(before * onehot, axis=1))


def rotation_tables(start, count, key_width):
    frequency = 1.0 / 10000.0 ** jnp.linspace(0.0, 1.0, key_width // 2, dtype=jnp.float32)
    token_position = (start + jnp.arange(count, dtype=jnp.int32)).astype(jnp.float32)
    angles = token_position[:, None] * frequency[None, :]
    return (jnp.cos(angles), jnp.sin(angles))


def turn(field, cosines, sines):
    paired = field.reshape(field.shape[:-1] + (field.shape[-1] // 2, 2))
    even_part = paired[..., 0]
    odd_part = paired[..., 1]
    cos_rows = cosines[:, None, :]
    sin_rows = sines[:, None, :]
    turned = jnp.stack(
        [even_part * cos_rows - odd_part * sin_rows, odd_part * cos_rows + even_part * sin_rows],
        axis=-1,
    )
    return turned.reshape(field.shape)


def decay_combine(earlier, next_rows):
    return (earlier[0] * next_rows[0], next_rows[1] + next_rows[0][:, None, None] * earlier[1])


MESH = pl.DeviceIdType.MESH
BF = jnp.bfloat16
F32 = jnp.float32


def dot(a, b, ca, cb, precision=None):
    return lax.dot_general(
        a, b, (((ca,), (cb,)), ((), ())), preferred_element_type=F32, precision=precision
    )


def place_of(p, x):
    return (p // 8, p // 2 % 4, p % 2, x)


def remote(src, dst, send_sem, recv_sem, device):
    pltpu.make_async_remote_copy(
        src_ref=src,
        dst_ref=dst,
        send_sem=send_sem,
        recv_sem=recv_sem,
        device_id=place_of(*device),
        device_id_type=MESH,
    ).start()


def take(ref, sem):
    pltpu.make_async_copy(ref, ref, sem).wait()


def expert_kernel(
    stream,
    og,
    routes,
    weight,
    gate_w,
    up_w,
    down_w,
    o_gate,
    o_up,
    o_down,
    o_resid,
    sq,
    oq,
    w,
    d,
    pm,
    send,
    rg,
    gu,
    ac,
    bk,
    xin,
    acc,
    fin,
    ret,
    rt,
    lsem,
    dsend,
    drecv,
    xsend,
    xrecv,
    rsend,
    rrecv,
    tsend,
    trecv,
    gsend,
    grecv,
):
    me = lax.axis_index(SP)
    x = lax.axis_index("tp")
    z, j = me // 8, me % 8
    right, left, far = (x + 1) % 4, (x + 3) % 4, (x + 2) % 4

    barrier = pltpu.get_barrier_semaphore()

    def hello(k, _):
        pl.semaphore_signal(
            barrier, inc=1, device_id=place_of((me + k) % 64, x), device_id_type=MESH
        )
        return 0

    lax.fori_loop(1, 64, hello, 0)
    for peer in (right, left, far):
        pl.semaphore_signal(barrier, inc=1, device_id=place_of(me, peer), device_id_type=MESH)

    cols = pl.ds(pl.multiple_of(x * 512, 512), 512)
    loads = [
        pltpu.make_async_copy(stream.at[:, cols], sq, lsem.at[0]),
        pltpu.make_async_copy(og.at[:, cols], oq, lsem.at[1]),
        pltpu.make_async_copy(gate_w.at[0], w.at[:, pl.ds(0, 256)], lsem.at[2]),
        pltpu.make_async_copy(up_w.at[0], w.at[:, pl.ds(256, 256)], lsem.at[3]),
        pltpu.make_async_copy(down_w.at[0], d, lsem.at[4]),
    ]
    for c in loads:
        c.start()

    ident = (
        lax.broadcasted_iota(jnp.int32, (128, 128), 0)
        == lax.broadcasted_iota(jnp.int32, (128, 128), 1)
    ).astype(F32)
    earlier = (
        lax.broadcasted_iota(jnp.int32, (128, 128), 0)
        < lax.broadcasted_iota(jnp.int32, (128, 128), 1)
    ).astype(BF)
    ids = dot(routes[...].astype(F32), ident, 0, 0)
    wrow = dot(weight[...], ident, 0, 0, lax.Precision.HIGHEST)
    expert = lax.broadcasted_iota(jnp.int32, (64, 128), 0).astype(F32)
    named0 = (expert == ids[0:1]).astype(F32)
    named1 = (expert == ids[1:2]).astype(F32)
    before = dot((named0 + named1).astype(BF), earlier, 1, 0)
    dest0 = ids[0:1] * 8.0 + jnp.sum(named0 * before, axis=0, keepdims=True)
    dest1 = ids[1:2] * 8.0 + jnp.sum(named1 * before, axis=0, keepdims=True)
    slot = lax.broadcasted_iota(jnp.int32, (512, 128), 0).astype(F32)
    at0 = (slot == dest0).astype(F32)
    at1 = (slot == dest1).astype(F32)
    wslot = jnp.sum(at0 * wrow[0:1] + at1 * wrow[1:2], axis=1, keepdims=True)
    place = (at0 + at1).astype(BF)
    pm[...] = place
    loads[0].wait()
    send[:, 0:8, :] = dot(place, sq[...], 1, 0).reshape(64, 8, 512).astype(BF)
    loads[1].wait()
    send[:, 8:16, :] = (dot(place, oq[...], 1, 0) * wslot).reshape(64, 8, 512).astype(BF)

    pl.semaphore_wait(barrier, 66)

    order = (0, 1, 7, 2, 6, 3, 5, 4)

    def plane(dz):
        return (z + dz) % 8

    def dispatch(dz):
        def one(k, _):
            p = plane(dz) * 8 + (j + k) % 8
            remote(send.at[p], rg.at[x, me], dsend, drecv.at[dz], (p, x))
            return 0

        lax.fori_loop(1 if dz == 0 else 0, 8, one, 0)

    for dz in order:
        dispatch(dz)
    rg[x, me] = send[me]

    def group(q, dz):
        return rg.at[q, pl.ds(plane(8 - dz) * 8, 8)]

    def half(q, dz, h):
        return rg.at[q, pl.ds(plane(8 - dz) * 8 + 4 * h, 4)]

    def spread(dz):
        if dz == 0:
            take(rg.at[0, pl.ds(0, 7)], drecv.at[0])
        else:
            take(rg.at[0, pl.ds(0, 8)], drecv.at[dz])
        remote(group(x, dz), group(x, dz), xsend, xrecv.at[0, dz], (me, right))
        remote(group(x, dz), group(x, dz), xsend, xrecv.at[1, dz], (me, left))

    def pass_on(dz):
        take(group(left, dz), xrecv.at[0, dz])
        remote(half(left, dz, 0), half(left, dz, 0), xsend, xrecv.at[2, dz], (me, right))
        take(group(right, dz), xrecv.at[1, dz])
        remote(half(right, dz, 1), half(right, dz, 1), xsend, xrecv.at[3, dz], (me, left))

    spread(order[0])
    for at, dz in enumerate(order):
        if at + 1 < 8:
            spread(order[at + 1])
        pass_on(dz)
    for dz in order:
        take(half(far, dz, 0), xrecv.at[2, dz])
        take(half(far, dz, 1), xrecv.at[3, dz])

    for c in loads[2:]:
        c.wait()

    pairs = ((1, 7), (2, 6), (3, 5), (4, 0))

    def experts(m):
        za, zb = plane(pairs[m][0]), plane(pairs[m][1])

        def both(q, part):
            rows = pl.ds(8 * part, 8)
            a = rg[q, pl.ds(za * 8, 8), rows, :].reshape(64, 512)
            b = rg[q, pl.ds(zb * 8, 8), rows, :].reshape(64, 512)
            return jnp.concatenate([a, b], axis=0)

        pre = dot(both(0, 0), w[0:512, :], 1, 0)
        back = dot(both(0, 1), d[:, 0:512], 1, 1)
        for q in range(1, 4):
            pre = pre + dot(both(q, 0), w[q * 512 : (q + 1) * 512, :], 1, 0)
            back = back + dot(both(q, 1), d[:, q * 512 : (q + 1) * 512], 1, 1)
        gate_pre, up_pre = pre[:, 0:256], pre[:, 256:512]
        gate_clip = jnp.minimum(gate_pre, CLAMP_LIMIT)
        up_clip = jnp.clip(up_pre, -CLAMP_LIMIT, CLAMP_LIMIT)
        sig = jax.nn.sigmoid(GATE_SLOPE * gate_clip)
        activated = (gate_clip * sig * (up_clip + 1.0)).astype(BF)
        slope = sig + GATE_SLOPE * gate_clip * sig * (1.0 - sig)
        gate_g = jnp.where(gate_pre < CLAMP_LIMIT, back * (up_clip + 1.0) * slope, 0.0).astype(BF)
        up_g = jnp.where(jnp.abs(up_pre) < CLAMP_LIMIT, back * gate_clip * sig, 0.0).astype(BF)
        both_g = jnp.concatenate([gate_g, up_g], axis=1)
        for part, zz in ((0, za), (1, zb)):
            at = pl.ds(pl.multiple_of(zz * 64, 64), 64)
            gu[at, :] = both_g[64 * part : 64 * part + 64]
            ac[at, :] = activated[64 * part : 64 * part + 64]
        for q in range(4):
            rows = dot(both_g, w[q * 512 : (q + 1) * 512, :], 1, 1).astype(BF)
            bk[q, pl.ds(za * 8, 8)] = rows[0:64].reshape(8, 8, 512)
            bk[q, pl.ds(zb * 8, 8)] = rows[64:128].reshape(8, 8, 512)

        pa, pb = pl.ds(za * 8, 8), pl.ds(zb * 8, 8)
        remote(bk.at[far, pa], xin.at[0, m], rsend, rrecv.at[0, m], (me, right))
        remote(bk.at[far, pb], xin.at[1, m], rsend, rrecv.at[1, m], (me, left))
        remote(bk.at[left, pa], xin.at[2, m], rsend, rrecv.at[2, m], (me, left))
        remote(bk.at[right, pb], xin.at[3, m], rsend, rrecv.at[3, m], (me, right))

    def forward(m):
        pa, pb = (pl.ds(plane(dz) * 8, 8) for dz in pairs[m])
        take(xin.at[0, m], rrecv.at[0, m])
        acc[0, m] = (xin[0, m].astype(F32) + bk[right, pa].astype(F32)).astype(BF)
        remote(acc.at[0, m], xin.at[4, m], rsend, rrecv.at[4, m], (me, right))
        take(xin.at[1, m], rrecv.at[1, m])
        acc[1, m] = (xin[1, m].astype(F32) + bk[left, pb].astype(F32)).astype(BF)
        remote(acc.at[1, m], xin.at[5, m], rsend, rrecv.at[5, m], (me, left))

    def finish(m):
        for part, dz in enumerate(pairs[m]):
            at = pl.ds(plane(dz) * 8, 8)
            direct, summed = 2 + part, 4 + part
            take(xin.at[direct, m], rrecv.at[direct, m])
            take(xin.at[summed, m], rrecv.at[summed, m])
            fin[at] = (
                bk[x, at].astype(F32) + xin[direct, m].astype(F32) + xin[summed, m].astype(F32)
            ).astype(BF)

            def one(k, _, dz=dz):
                p = plane(dz) * 8 + (j + k) % 8
                remote(fin.at[p], ret.at[me], tsend, trecv, (p, x))
                return 0

            lax.fori_loop(1 if dz == 0 else 0, 8, one, 0)
            if dz == 0:
                ret[me] = fin[me]

    def weight_grads(q):
        at = pl.ds(q * 512, 512)
        rows = rg[q, :, 0:8, :].reshape(512, 512)
        grads = rg[q, :, 8:16, :].reshape(512, 512)
        both = dot(rows, gu[...], 0, 0).astype(BF)
        o_gate[at, :] = both[:, 0:256]
        o_up[at, :] = both[:, 256:512]
        o_down[:, at] = dot(ac[...], grads, 0, 0).astype(BF)

    for m in range(4):
        experts(m)
        if m >= 1:
            forward(m - 1)
    forward(3)
    for m in range(4):
        finish(m)
        weight_grads(m)

    take(ret.at[pl.ds(0, 63)], trecv)
    resid = dot(ret[...].reshape(512, 512), pm[...], 0, 0) + dot(oq[...], ident.astype(BF), 0, 0)
    rt[x] = resid.astype(BF)
    for k, peer in enumerate((right, left, far)):
        remote(rt.at[x], rt.at[x], gsend, grecv.at[k], (me, peer))
    for k, peer in enumerate((left, right, far)):
        take(rt.at[peer], grecv.at[k])
    o_resid[...] = rt[...].reshape(2048, 128)

    take(send.at[pl.ds(0, 63)], dsend)
    take(rg.at[pl.ds(0, 3)], xsend)
    take(xin, rsend)
    take(fin.at[pl.ds(0, 63)], tsend)
    take(rt.at[pl.ds(0, 3)], gsend)


def expert_call(stream, out_grad, routes, route_weight, gate_weight, up_weight, down_weight):
    anywhere = pl.BlockSpec(memory_space=pl.ANY)
    local = pl.BlockSpec(memory_space=pltpu.VMEM)
    dma = pltpu.SemaphoreType.DMA
    return pl.pallas_call(
        expert_kernel,
        out_shape=(
            jax.ShapeDtypeStruct((2048, 256), BF),
            jax.ShapeDtypeStruct((2048, 256), BF),
            jax.ShapeDtypeStruct((256, 2048), BF),
            jax.ShapeDtypeStruct((2048, 128), BF),
        ),
        in_specs=[anywhere, anywhere, local, local, anywhere, anywhere, anywhere],
        out_specs=(local, local, local, local),
        scratch_shapes=[
            pltpu.VMEM((128, 512), BF),
            pltpu.VMEM((128, 512), BF),
            pltpu.VMEM((2048, 512), BF),
            pltpu.VMEM((256, 2048), BF),
            pltpu.VMEM((512, 128), BF),
            pltpu.VMEM((64, 16, 512), BF),
            pltpu.VMEM((4, 64, 16, 512), BF),
            pltpu.VMEM((512, 512), BF),
            pltpu.VMEM((512, 256), BF),
            pltpu.VMEM((4, 64, 8, 512), BF),
            pltpu.VMEM((6, 4, 8, 8, 512), BF),
            pltpu.VMEM((2, 4, 8, 8, 512), BF),
            pltpu.VMEM((64, 8, 512), BF),
            pltpu.VMEM((64, 8, 512), BF),
            pltpu.VMEM((4, 512, 128), BF),
            dma((5,)),
            dma,
            dma((8,)),
            dma,
            dma((4, 8)),
            dma,
            dma((6, 4)),
            dma,
            dma,
            dma,
            dma((3,)),
        ],
        compiler_params=pltpu.CompilerParams(
            collective_id=0, has_side_effects=True, vmem_limit_bytes=60 * 1024 * 1024
        ),
    )(stream, out_grad, routes, route_weight, gate_weight, up_weight, down_weight)


def per_device(
    stream,
    out_grad,
    routes,
    route_weight,
    queries,
    key_vectors,
    value_vectors,
    log_decay,
    out_proj,
    gate_weight,
    up_weight,
    down_weight,
):
    tokens_here = stream.shape[0]
    gate_part, up_part, down_part, resid_t = expert_call(
        stream, out_grad, routes, route_weight, gate_weight, up_weight, down_weight
    )
    heads_local = queries.shape[1]
    key_width = queries.shape[2]
    value_width = value_vectors.shape[2]
    key_scale = key_width ** (-0.5)
    cosines, sines = rotation_tables(lax.axis_index(SP) * tokens_here, tokens_here, key_width)
    query_rotated = turn(queries.astype(jnp.float32), cosines, sines).transpose(1, 0, 2)
    key_rotated = (turn(key_vectors.astype(jnp.float32), cosines, sines) * key_scale).transpose(
        1, 0, 2
    )
    value_per_head = value_vectors.astype(jnp.float32).transpose(1, 0, 2)
    running_total = jnp.cumsum(log_decay, axis=0).T
    block_total = running_total[:, -1]
    causal = (jnp.arange(tokens_here)[:, None] >= jnp.arange(tokens_here)[None, :])[None]
    difference = running_total[:, :, None] - running_total[:, None, :]
    decay_mask = jnp.where(causal, jnp.exp(jnp.where(causal, difference, 0.0)), 0.0)
    per_head_decay = jnp.exp(running_total)
    remaining_decay = jnp.exp(block_total[:, None] - running_total)
    carried = jnp.exp(block_total)
    inner_state = jnp.einsum(
        "wfs,wfi->wsi",
        key_rotated * remaining_decay[..., None],
        value_per_head,
        precision=TOP_PRECISION,
    )
    identity = (jnp.ones_like(carried), jnp.zeros_like(inner_state))
    incoming_state = prefix_by_axis((carried, inner_state), SP, decay_combine, identity)[1]
    weights = (
        jnp.einsum("hik,hjk->hij", query_rotated, key_rotated, precision=TOP_PRECISION) * decay_mask
    )
    retained_output = jnp.einsum("hij,hjv->hiv", weights, value_per_head, precision=TOP_PRECISION)
    retained_output = retained_output + per_head_decay[..., None] * jnp.einsum(
        "dzr,drs->dzs", query_rotated, incoming_state, precision=TOP_PRECISION
    )
    inverse_rms = lax.rsqrt(
        jnp.mean(retained_output * retained_output, axis=-1, keepdims=True) + EPSILON
    )
    normed = retained_output * inverse_rms
    normed_bf = (
        normed.transpose(1, 0, 2)
        .reshape(tokens_here, heads_local * value_width)
        .astype(jnp.bfloat16)
    )
    proj_grad = summed_rows(
        lax.dot_general(
            resid_t, normed_bf, (((1,), (0,)), ((), ())), preferred_element_type=jnp.float32
        ),
        SP,
    )
    normed_grad = lax.dot_general(
        resid_t, out_proj, (((0,), (0,)), ((), ())), preferred_element_type=jnp.float32
    )
    normed_grad = normed_grad.reshape(tokens_here, heads_local, value_width).transpose(1, 0, 2)
    retention_gradient = inverse_rms * (
        normed_grad - normed * jnp.mean(normed_grad * normed, axis=-1, keepdims=True)
    )
    inner_gradient = jnp.einsum(
        "gwn,gwj->gnj",
        query_rotated * per_head_decay[..., None],
        retention_gradient,
        precision=TOP_PRECISION,
    )
    future_gradient = prefix_by_axis_2((carried, inner_gradient), SP, decay_combine, identity)[1]
    score_grad = (
        jnp.einsum("hiv,hjv->hij", retention_gradient, value_per_head, precision=TOP_PRECISION)
        * decay_mask
    )
    query_portion = jnp.einsum("hij,hjk->hik", score_grad, key_rotated, precision=TOP_PRECISION)
    query_portion = query_portion + per_head_decay[..., None] * jnp.einsum(
        "bpl,btl->bpt", retention_gradient, incoming_state, precision=TOP_PRECISION
    )
    key_portion = jnp.einsum("hij,hik->hjk", score_grad, query_rotated, precision=TOP_PRECISION)
    key_portion = key_portion + remaining_decay[..., None] * jnp.einsum(
        "uxn,ubn->uxb", value_per_head, future_gradient, precision=TOP_PRECISION
    )
    value_portion = jnp.einsum("hij,hiv->hjv", weights, retention_gradient, precision=TOP_PRECISION)
    value_portion = value_portion + remaining_decay[..., None] * jnp.einsum(
        "bui,bim->bum", key_rotated, future_gradient, precision=TOP_PRECISION
    )
    query_grad = turn(query_portion.transpose(1, 0, 2), cosines, -sines).astype(jnp.bfloat16)
    key_grad = (turn(key_portion.transpose(1, 0, 2), cosines, -sines) * key_scale).astype(
        jnp.bfloat16
    )
    value_grad = value_portion.transpose(1, 0, 2).astype(jnp.bfloat16)
    return (
        gate_part[None],
        up_part[None],
        down_part[None],
        proj_grad,
        query_grad,
        key_grad,
        value_grad,
    )


def solution(mesh):
    split = Mesh(mesh.devices.reshape(8, 4, 2, mesh.shape["tp"]), ("sp_0", "sp_1", "sp_2", "tp"))
    placed = (
        P(SP, None),
        P(SP, None),
        P(SP, None),
        P(SP, None),
        P(SP, "tp", None),
        P(SP, "tp", None),
        P(SP, "tp", None),
        P(SP, "tp"),
        P(None, "tp"),
        P(SP, None, "tp"),
        P(SP, None, "tp"),
        P(SP, "tp", None),
    )
    return jax.shard_map(
        per_device,
        mesh=split,
        in_specs=placed,
        out_specs=(
            P(SP, None, "tp"),
            P(SP, None, "tp"),
            P(SP, "tp", None),
            P(SP, "tp"),
            P(SP, "tp", None),
            P(SP, "tp", None),
            P(SP, "tp", None),
        ),
        check_vma=False,
    )
```

```python
import types

import jax
import jax.numpy as jnp
import numpy as np
from jax import lax
from jax.experimental import pallas as pl
from jax.experimental.pallas import tpu as pltpu
from jax.sharding import PartitionSpec as P

CLAMP_LIMIT = 7.0
GATE_SLOPE = 1.702
EPSILON = 1e-06
MESH = pl.DeviceIdType.MESH
BF = jnp.bfloat16
F32 = jnp.float32
HIGHEST = lax.Precision.HIGHEST

N_SP, N_TP = 64, 4
TOK, D, KD, VD = 128, 2048, 128, 256
QUART = D // N_TP
SHIFTS = (1, 7, 2, 6, 3, 5, 4)
WHOLE = (1, 7, 0)
BOTH = (1, 7)
PARTS = (1, 7, 2, 6, 3, 5, 4)
QUEUE = (
    (1, False),
    (7, False),
    (2, False),
    (6, False),
    (1, True),
    (7, True),
    (3, False),
    (5, False),
    (0, True),
    (4, False),
)
FIRST = 0
CHUNKS = (
    ((1, 0, 8), (7, 0, 8)),
    ((2, 0, 8), (6, 0, 8)),
    ((0, 0, 4), (0, 4, 4)),
    ((3, 0, 8), (5, 0, 8)),
    ((4, 0, 4), (4, 4, 4)),
)


def dot(a, b, ca, cb, precision=None):
    return lax.dot_general(
        a, b, (((ca,), (cb,)), ((), ())), preferred_element_type=F32, precision=precision
    )


def dotb(a, b, ca, cb):
    return dot(a.astype(BF), b.astype(BF), ca, cb)


def remote(src, dst, send_sem, recv_sem, device):
    pltpu.make_async_remote_copy(
        src_ref=src,
        dst_ref=dst,
        send_sem=send_sem,
        recv_sem=recv_sem,
        device_id=device,
        device_id_type=MESH,
    ).start()


def take(ref, sem):
    pltpu.make_async_copy(ref, ref, sem).wait()


def iota(shape, dim):
    return lax.broadcasted_iota(jnp.int32, shape, dim)


INPUTS = (
    "stream",
    "og",
    "in_routes",
    "in_weight",
    "in_queries",
    "in_keys",
    "in_values",
    "in_decay",
    "out_proj",
    "gate_w",
    "up_w",
    "down_w",
    "in_starts",
    "in_places",
)
SMALL = {
    "routes": ((2, TOK), jnp.int32),
    "weight": ((2, TOK), F32),
    "decay": ((2, TOK), F32),
    "starts": ((2 * N_SP, KD), F32),
    "places": ((2 * TOK, KD), F32),
    "queries": ((TOK, 2, KD), BF),
    "keys": ((TOK, 2, KD), BF),
    "values": ((TOK, 2, VD), BF),
}
OUTPUTS = {
    "o_gate": ((1, D, 256), BF),
    "o_up": ((1, D, 256), BF),
    "o_down": ((1, 256, D), BF),
    "o_proj": ((32, 512), F32),
    "o_query": ((TOK, 2, KD), BF),
    "o_key": ((TOK, 2, KD), BF),
    "o_value": ((TOK, 2, VD), BF),
}
BUFFERS = {
    **SMALL,
    "sf": ((TOK, D), BF),
    "of": ((TOK, D), BF),
    "ws": ((512, 1), F32),
    "w": ((D, 512), BF),
    "d": ((256, D), BF),
    "op": ((D, 512), BF),
    "pm": ((512, TOK), BF),
    "send": ((N_SP, 16, QUART), BF),
    "whole": ((3, 8, 4, 16, QUART), BF),
    "rg": ((N_SP, 4, 16, QUART), BF),
    "gu": ((512, 512), BF),
    "ac": ((512, 256), BF),
    "bk": ((4, N_SP, 8, QUART), BF),
    "xin": ((6, 5, 8, 8, QUART), BF),
    "acc": ((2, 5, 8, 8, QUART), BF),
    "fin": ((N_SP, 8, QUART), BF),
    "ret": ((N_SP, 8, QUART), BF),
    "rt": ((N_SP, 32, TOK), BF),
    "qr": ((2, TOK, KD), F32),
    "kr": ((2, TOK, KD), F32),
    "vh": ((2, TOK, VD), BF),
    "mask": ((2, TOK, TOK), F32),
    "wt": ((2, TOK, TOK), BF),
    "nrm": ((2, TOK, VD), F32),
    "inv": ((2, TOK, 1), F32),
    "phd": ((2, TOK, 1), F32),
    "rem": ((2, TOK, 1), F32),
    "sa": ((2, 8, 32, VD), BF),
    "ra": ((2, 8, 32, VD), BF),
    "pp": ((2, 8, 32, VD), F32),
    "sb": ((2, 32, VD), BF),
    "rb": ((2, 8, 32, VD), BF),
    "sc": ((2, 8, 32, VD), BF),
    "rc": ((2, 8, 32, VD), BF),
    "tmine": ((2, VD), F32),
    "tplane": ((2, VD), F32),
    "ta": ((8, 2, VD), F32),
    "tb": ((8, 2, VD), F32),
    "nb": ((TOK, 512), BF),
    "na": ((8, TOK, 512), BF),
    "rr": ((8, 8, 32, TOK), BF),
    "zp": ((8, 32, 512), BF),
    "rz": ((8, 32, 512), BF),
}
SEMAPHORES = {
    "load": (14,),
    "d_send": (),
    "d_recv": (2, 8),
    "x_send": (),
    "x_recv": (4, 8),
    "r_send": (),
    "r_recv": (6, 5),
    "t_send": (),
    "t_recv": (),
    "g_send": (),
    "g_recv": (6,),
    "s_send": (2, 3),
    "s_recv": (2, 3),
    "u_send": (2,),
    "u_recv": (2,),
    "n_send": (),
    "n_recv": (3,),
    "p_send": (2,),
    "p_recv": (),
    "q_recv": (4,),
}
NAMES = (*INPUTS, *OUTPUTS, *BUFFERS, *SEMAPHORES)


def kernel(*refs):
    r = types.SimpleNamespace(**dict(zip(NAMES, refs, strict=True)))
    me = lax.axis_index("sp")
    x = lax.axis_index("tp")
    z, j = me // 8, me % 8
    other = j + 1 - 2 * (j % 2)
    right, left, far = (x + 1) % 4, (x + 3) % 4, (x + 2) % 4

    def plane(dz):
        return (z + dz) % 8

    cols = pl.ds(pl.multiple_of(x * QUART, QUART), QUART)
    barrier = pltpu.get_barrier_semaphore()

    def hello(k, _):
        pl.semaphore_signal(barrier, inc=1, device_id=((me + k) % 64, x), device_id_type=MESH)
        return 0

    lax.fori_loop(32, 64, hello, 0)
    lax.fori_loop(1, 32, hello, 0)
    for peer in (right, left, far):
        pl.semaphore_signal(barrier, inc=1, device_id=(me, peer), device_id_type=MESH)

    copies = [
        (r.in_routes, r.routes),
        (r.in_weight, r.weight),
        (r.stream, r.sf),
        (r.og, r.of),
        *((getattr(r, "in_" + name), getattr(r, name)) for name in list(SMALL)[2:]),
        (r.gate_w.at[0], r.w.at[:, pl.ds(0, 256)]),
        (r.up_w.at[0], r.w.at[:, pl.ds(256, 256)]),
        (r.down_w.at[0], r.d),
        (r.out_proj, r.op),
    ]
    loads = [pltpu.make_async_copy(*c, r.load.at[i]) for i, c in enumerate(copies)]
    for c in loads:
        c.start()

    rows, lanes = iota((TOK, TOK), 0), iota((TOK, TOK), 1)
    loads[0].wait()
    loads[1].wait()
    ids = r.routes[...].astype(F32)
    wrow = r.weight[...]
    expert = iota((64, TOK), 0).astype(F32)
    named0 = (expert == ids[0:1]).astype(F32)
    named1 = (expert == ids[1:2]).astype(F32)
    before = dotb(named0 + named1, (rows < lanes).astype(F32), 1, 0)
    dest0 = ids[0:1] * 8.0 + jnp.sum(named0 * before, axis=0, keepdims=True)
    dest1 = ids[1:2] * 8.0 + jnp.sum(named1 * before, axis=0, keepdims=True)
    slot = iota((512, TOK), 0).astype(F32)
    at0 = (slot == dest0).astype(F32)
    at1 = (slot == dest1).astype(F32)
    wslot = jnp.sum(at0 * wrow[0:1] + at1 * wrow[1:2], axis=1, keepdims=True)
    place = (at0 + at1).astype(BF)
    r.pm[...] = place
    r.ws[...] = wslot
    loads[2].wait()
    r.send[:, 0:8, :] = dot(place, r.sf[:, cols], 1, 0).reshape(64, 8, QUART).astype(BF)
    loads[3].wait()
    r.send[:, 8:16, :] = (dot(place, r.of[:, cols], 1, 0) * wslot).reshape(64, 8, QUART).astype(BF)

    pl.semaphore_wait(barrier, 66)

    mine, others = j // 4 * 4, 4 - j // 4 * 4

    def dispatch(dz, whole):
        def send_to(m):
            p = plane(dz) * 8 + m
            if whole:
                block, slot_of = r.whole.at[WHOLE.index(dz), m], r.rg.at[me]
            else:
                block, slot_of = r.send.at[p], r.rg.at[me, x]
            remote(block, slot_of, r.d_send, r.d_recv.at[int(whole), dz], (p, x))

        def one(k, _):
            send_to((j + k) % 8)
            return 0

        def one_of_half(k, _):
            send_to((mine if whole else others) + (j + k) % 4)
            return 0

        if dz in BOTH:
            lax.fori_loop(0, 4, one_of_half, 0)
        else:
            lax.fori_loop(1 if dz == 0 else 0, 8, one, 0)

    def build_whole():
        for i, dz in enumerate(WHOLE):
            at = pl.ds(pl.multiple_of(plane(dz) * 64, 64), 64)
            slots, scale = r.pm[at, :], r.ws[at, :]
            for q in range(4):
                these = slice(q * QUART, (q + 1) * QUART)
                rows_q = dot(slots, r.sf[:, these], 1, 0)
                grads_q = dot(slots, r.of[:, these], 1, 0) * scale
                r.whole[i, :, q, 0:8, :] = rows_q.reshape(8, 8, QUART).astype(BF)
                r.whole[i, :, q, 8:16, :] = grads_q.reshape(8, 8, QUART).astype(BF)

    first_whole = [whole for _, whole in QUEUE].index(True)
    for at, (dz, whole) in enumerate(QUEUE):
        if at == first_whole:
            build_whole()
        dispatch(dz, whole)
    r.rg[me] = r.whole[WHOLE.index(0), j]

    odd = lanes % 2 == 1

    def angles():
        ca, sa = r.starts[pl.ds(me, 1), :], r.starts[pl.ds(me + 64, 1), :]
        cb, sb = r.places[0:128, :], r.places[128:256, :]
        return ca * cb - sa * sb, jnp.where(odd, 1.0, -1.0) * (sa * cb + ca * sb)

    def turn(field, cosines, sines):
        partner = jnp.where(odd, pltpu.roll(field, 1, 1), pltpu.roll(field, TOK - 1, 1))
        return field * cosines + partner * sines

    def apart():
        a, b = iota((256, 256), 0), iota((256, 256), 1)
        return (b == 2 * (a % 128) + a // 128).astype(BF)

    for c in loads[4:10]:
        c.wait()
    cosines, sines = angles()
    split = apart()
    q2 = dot(split, r.queries[...].reshape(256, KD), 1, 0)
    k2 = dot(split, r.keys[...].reshape(256, KD), 1, 0)
    v2 = [dot(split, r.values[:, :, 128 * i : 128 * i + 128].reshape(256, 128), 1, 0) for i in (0, 1)]
    decay = r.decay[...]
    cum_row = dot(decay, (rows <= lanes).astype(F32), 1, 0, HIGHEST)
    cum_col = dot((rows >= lanes).astype(F32), decay, 1, 1, HIGHEST)
    causal = rows >= lanes
    for h in range(2):
        at = slice(128 * h, 128 * h + 128)
        q = turn(q2[at], cosines, sines)
        k = turn(k2[at], cosines, sines) * KD ** (-0.5)
        r.qr[h] = q
        r.kr[h] = k
        r.vh[h, :, 0:128] = v2[0][at].astype(BF)
        r.vh[h, :, 128:256] = v2[1][at].astype(BF)
        col = cum_col[:, h : h + 1]
        total = cum_col[127:128, h : h + 1]
        rem = jnp.exp(total - col)
        r.phd[h] = jnp.exp(col)
        r.rem[h] = rem
        diff = col - cum_row[h : h + 1, :]
        mask = jnp.where(causal, jnp.exp(jnp.where(causal, diff, 0.0)), 0.0)
        r.mask[h] = mask
        state = dotb(k * rem, r.vh[h], 0, 0)
        r.sa[0, pl.ds(4 * h, 4)] = state.astype(BF).reshape(4, 32, VD)
        r.tmine[h : h + 1, :] = jnp.broadcast_to(total, (1, VD))

    def within(src, dst, send_sem, recv_sem):
        def one(k, _):
            m = (j + k) % 8
            remote(src(m), dst(j), send_sem, recv_sem, (z * 8 + m, x))
            return 0

        lax.fori_loop(1, 8, one, 0)

    def over_z(src, dst, send_sem, recv_sem):
        for dz in PARTS:
            remote(src(plane(dz)), dst(z), send_sem, recv_sem, (plane(dz) * 8 + j, x))

    def stage_a(way):
        within(
            lambda m: r.sa.at[way, m],
            lambda m: r.ra.at[way, m],
            r.s_send.at[way, 0],
            r.s_recv.at[way, 0],
        )
        r.ra[way, j] = r.sa[way, j]
        if way == 0:
            within(lambda m: r.tmine, lambda m: r.ta.at[m], r.u_send.at[0], r.u_recv.at[0])
            r.ta[j] = r.tmine[...]

    head = pl.ds(j // 4, 1)

    def stage_b(way):
        take(r.ra.at[way, pl.ds(0, 7)], r.s_recv.at[way, 0])
        if way == 0:
            take(r.ta.at[pl.ds(0, 7)], r.u_recv.at[0])
            total = r.ta[0]
            for m in range(1, 8):
                total = total + r.ta[m]
            r.tplane[...] = total
        run = jnp.zeros((32, VD), F32)
        for m in range(8) if way == 0 else reversed(range(8)):
            r.pp[way, m] = run
            run = jnp.exp(r.ta[m, head, :]) * run + r.ra[way, m].astype(F32)
        r.sb[way] = run.astype(BF)
        over_z(
            lambda p: r.sb.at[way],
            lambda p: r.rb.at[way, p],
            r.s_send.at[way, 1],
            r.s_recv.at[way, 1],
        )
        r.rb[way, z] = r.sb[way]
        if way == 0:
            over_z(lambda p: r.tplane, lambda p: r.tb.at[p], r.u_send.at[1], r.u_recv.at[1])
            r.tb[z] = r.tplane[...]

    def stage_c(way):
        take(r.rb.at[way, pl.ds(0, 7)], r.s_recv.at[way, 1])
        if way == 0:
            take(r.tb.at[pl.ds(0, 7)], r.u_recv.at[1])
        run = jnp.zeros((32, VD), F32)
        for p in range(8) if way == 0 else reversed(range(8)):
            passed = (p < z) if way == 0 else (p > z)
            new = jnp.exp(r.tb[p, head, :]) * run + r.rb[way, p].astype(F32)
            run = jnp.where(passed, new, run)
        logs = jnp.zeros((1, VD), F32)
        for m in range(8) if way == 0 else reversed(range(8)):
            r.sc[way, m] = (jnp.exp(logs) * run + r.pp[way, m]).astype(BF)
            logs = logs + r.ta[m, head, :]
        within(
            lambda m: r.sc.at[way, m],
            lambda m: r.rc.at[way, m],
            r.s_send.at[way, 2],
            r.s_recv.at[way, 2],
        )
        r.rc[way, j] = r.sc[way, j]

    def state_of(way, h):
        return r.rc[way, pl.ds(4 * h, 4)].reshape(128, VD)

    def normalise():
        take(r.rc.at[0, pl.ds(0, 7)], r.s_recv.at[0, 2])
        for h in range(2):
            q, k, v = r.qr[h], r.kr[h], r.vh[h]
            weights = (dotb(q, k, 1, 1) * r.mask[h]).astype(BF)
            r.wt[h] = weights
            kept = dot(weights, v, 1, 0) + r.phd[h] * dotb(q, state_of(0, h), 1, 0)
            inv = lax.rsqrt(jnp.mean(kept * kept, axis=1, keepdims=True) + EPSILON)
            r.inv[h] = inv
            r.nrm[h] = kept * inv
            r.nb[:, 256 * h : 256 * h + 256] = (kept * inv).astype(BF)
        r.na[j] = r.nb[...]
        remote(r.nb, r.na.at[j], r.n_send, r.n_recv.at[0], (z * 8 + other, x))
        for k in range(1, 4):
            m = (j + 2 * k) % 8
            remote(r.nb, r.na.at[j], r.n_send, r.n_recv.at[1], (z * 8 + m, x))

    def relay():
        take(r.na.at[pl.ds(0, 3)], r.n_recv.at[1])
        for k in range(1, 4):
            m = (j + 2 * k) % 8
            remote(r.na.at[m], r.na.at[m], r.n_send, r.n_recv.at[2], (z * 8 + other, x))

    def senders(dz):
        if dz in BOTH:
            return plane(8 - dz) * 8 + others, 4
        return plane(8 - dz) * 8, 8

    def group(q, dz):
        first, n = senders(dz)
        return r.rg.at[pl.ds(first, n), q]

    def half(q, dz, h):
        first, n = senders(dz)
        return r.rg.at[pl.ds(first + h * (n // 2), n // 2), q]

    def spread(dz):
        take(group(x, dz), r.d_recv.at[0, dz])
        remote(group(x, dz), group(x, dz), r.x_send, r.x_recv.at[0, dz], (me, right))
        remote(group(x, dz), group(x, dz), r.x_send, r.x_recv.at[1, dz], (me, left))

    def pass_on(dz):
        take(group(left, dz), r.x_recv.at[0, dz])
        remote(half(left, dz, 0), half(left, dz, 0), r.x_send, r.x_recv.at[2, dz], (me, right))
        take(group(right, dz), r.x_recv.at[1, dz])
        remote(half(right, dz, 1), half(right, dz, 1), r.x_send, r.x_recv.at[3, dz], (me, left))

    def complete(dz):
        if dz in PARTS:
            take(half(far, dz, 0), r.x_recv.at[2, dz])
            take(half(far, dz, 1), r.x_recv.at[3, dz])
        if dz in BOTH:
            take(r.rg.at[pl.ds(plane(8 - dz) * 8 + mine, 4)], r.d_recv.at[1, dz])
        elif dz in WHOLE:
            take(r.rg.at[pl.ds(0, 7)], r.d_recv.at[1, dz])

    def block(m, part):
        dz, first, n = CHUNKS[m][part]
        return plane(8 - dz) * 8 + first, n

    def experts(m):
        for dz in dict.fromkeys(c[0] for c in CHUNKS[m]):
            complete(dz)
        if m == FIRST:
            for c in loads[10:]:
                c.wait()
        (fa, na), (fb, nb) = block(m, 0), block(m, 1)

        def both(q, part):
            these = pl.ds(8 * part, 8)
            a = r.rg[pl.ds(fa, na), q, these, :].reshape(8 * na, QUART)
            b = r.rg[pl.ds(fb, nb), q, these, :].reshape(8 * nb, QUART)
            return jnp.concatenate([a, b], axis=0)

        pre = dot(both(0, 0), r.w[0:QUART, :], 1, 0)
        back = dot(both(0, 1), r.d[:, 0:QUART], 1, 1)
        for q in range(1, 4):
            pre = pre + dot(both(q, 0), r.w[q * QUART : (q + 1) * QUART, :], 1, 0)
            back = back + dot(both(q, 1), r.d[:, q * QUART : (q + 1) * QUART], 1, 1)
        gate_pre, up_pre = pre[:, 0:256], pre[:, 256:512]
        gate_clip = jnp.minimum(gate_pre, CLAMP_LIMIT)
        up_clip = jnp.clip(up_pre, -CLAMP_LIMIT, CLAMP_LIMIT)
        sig = jax.nn.sigmoid(GATE_SLOPE * gate_clip)
        activated = (gate_clip * sig * (up_clip + 1.0)).astype(BF)
        slope = sig + GATE_SLOPE * gate_clip * sig * (1.0 - sig)
        gate_g = jnp.where(gate_pre < CLAMP_LIMIT, back * (up_clip + 1.0) * slope, 0.0).astype(BF)
        up_g = jnp.where(jnp.abs(up_pre) < CLAMP_LIMIT, back * gate_clip * sig, 0.0).astype(BF)
        both_g = jnp.concatenate([gate_g, up_g], axis=1)
        for lo, first, n in ((0, fa, na), (8 * na, fb, nb)):
            at = pl.ds(pl.multiple_of(first * 8, 32), 8 * n)
            r.gu[at, :] = both_g[lo : lo + 8 * n]
            r.ac[at, :] = activated[lo : lo + 8 * n]
        for q in range(4):
            out = dot(both_g, r.w[q * QUART : (q + 1) * QUART, :], 1, 1).astype(BF)
            for lo, first, n in ((0, fa, na), (8 * na, fb, nb)):
                r.bk[q, pl.ds(first, n)] = out[lo : lo + 8 * n].reshape(n, 8, QUART)

        pa, pb = pl.ds(fa, na), pl.ds(fb, nb)
        for k, rows_of, to in (
            (0, r.bk.at[far, pa], right),
            (1, r.bk.at[far, pb], left),
            (2, r.bk.at[left, pa], left),
            (3, r.bk.at[right, pb], right),
        ):
            space = r.xin.at[k, m, pl.ds(0, nb if k % 2 else na)]
            remote(rows_of, space, r.r_send, r.r_recv.at[k, m], (me, to))

    def forward(m):
        for part, mine_of, to in ((0, right, right), (1, left, left)):
            first, n = block(m, part)
            at, here = pl.ds(0, n), pl.ds(first, n)
            take(r.xin.at[part, m, at], r.r_recv.at[part, m])
            r.acc[part, m, at] = (
                r.xin[part, m, at].astype(F32) + r.bk[mine_of, here].astype(F32)
            ).astype(BF)
            remote(
                r.acc.at[part, m, at],
                r.xin.at[4 + part, m, at],
                r.r_send,
                r.r_recv.at[4 + part, m],
                (me, to),
            )

    def finish(m):
        for part in range(2):
            dz = CHUNKS[m][part][0]
            first, n = block(m, part)
            at, here = pl.ds(0, n), pl.ds(first, n)
            direct, summed = 2 + part, 4 + part
            take(r.xin.at[direct, m, at], r.r_recv.at[direct, m])
            take(r.xin.at[summed, m, at], r.r_recv.at[summed, m])
            r.fin[here] = (
                r.bk[x, here].astype(F32)
                + r.xin[direct, m, at].astype(F32)
                + r.xin[summed, m, at].astype(F32)
            ).astype(BF)

            def one(k, _, first=first, n=n, dz=dz):
                p = first + (j + k) % n
                if dz == 0:

                    @pl.when(p != me)
                    def _():
                        remote(r.fin.at[p], r.ret.at[me], r.t_send, r.t_recv, (p, x))

                else:
                    remote(r.fin.at[p], r.ret.at[me], r.t_send, r.t_recv, (p, x))
                return 0

            lax.fori_loop(0, n, one, 0)
            if dz == 0:

                @pl.when((me >= first) & (me < first + n))
                def _():
                    r.ret[me] = r.fin[me]

    def weight_grads(q):
        at = pl.ds(q * QUART, QUART)
        rows_q = r.rg[:, q, 0:8, :].reshape(512, QUART)
        grads_q = r.rg[:, q, 8:16, :].reshape(512, QUART)
        both = dot(rows_q, r.gu[...], 0, 0).astype(BF)
        r.o_gate[0, at, :] = both[:, 0:256]
        r.o_up[0, at, :] = both[:, 256:512]
        r.o_down[0, :, at] = dot(r.ac[...], grads_q, 0, 0).astype(BF)

    spread(1)
    spread(7)
    stage_a(0)
    pass_on(1)
    pass_on(7)
    spread(2)
    spread(6)
    pass_on(2)
    pass_on(6)
    experts(0)
    spread(3)
    forward(0)
    spread(5)
    pass_on(3)
    experts(1)
    pass_on(5)
    finish(0)
    spread(4)
    forward(1)
    stage_b(0)
    experts(2)
    experts(3)
    pass_on(4)
    finish(1)
    stage_c(0)
    forward(2)
    forward(3)
    experts(4)
    finish(2)
    normalise()
    finish(3)
    weight_grads(0)
    forward(4)
    weight_grads(1)
    finish(4)
    relay()
    weight_grads(2)
    weight_grads(3)

    def quarter(q):
        return pl.ds(q * 16, 16)

    take(r.ret.at[pl.ds(0, 63)], r.t_recv)
    same = (rows == lanes).astype(BF)
    resid = dot(r.ret[...].reshape(512, QUART), r.pm[...], 0, 0) + dot(r.of[:, cols], same, 0, 0)
    r.rt[quarter(x)] = resid.astype(BF).reshape(16, 32, TOK)
    def part_of(q, h):
        return r.rt.at[pl.ds(q * 16 + 8 * h, 8)]

    for k, (h, peer) in enumerate(((0, right), (1, left), (1, right), (0, left))):
        remote(part_of(x, h), part_of(x, h), r.g_send, r.g_recv.at[k], (me, peer))

    def give(i, q):
        def one(k, _):
            m = (j + k) % 8
            for p in (2 * q, 2 * q + 1):
                remote(
                    r.rt.at[p * 8 + m],
                    r.rr.at[j, p],
                    r.p_send.at[0],
                    r.q_recv.at[i],
                    (z * 8 + m, x),
                )
            return 0

        lax.fori_loop(1, 8, one, 0)
        for p in (2 * q, 2 * q + 1):
            r.rr[j, p] = r.rt[p * 8 + j]

    give(0, x)

    def share(q):
        rows_q = pl.ds(pl.multiple_of(q * QUART, QUART), QUART)
        return dot(r.rt[quarter(q)].reshape(QUART, TOK), r.op[rows_q, :], 0, 0)

    take(part_of(left, 0), r.g_recv.at[0])
    remote(part_of(left, 0), part_of(left, 0), r.g_send, r.g_recv.at[4], (me, right))
    take(part_of(right, 1), r.g_recv.at[1])
    remote(part_of(right, 1), part_of(right, 1), r.g_send, r.g_recv.at[5], (me, left))
    take(part_of(left, 1), r.g_recv.at[2])
    take(part_of(right, 0), r.g_recv.at[3])
    give(1, left)
    give(2, right)
    normed_grad = share(x) + share(left) + share(right)
    take(part_of(far, 0), r.g_recv.at[4])
    take(part_of(far, 1), r.g_recv.at[5])
    normed_grad = normed_grad + share(far)

    grads = []
    for h in range(2):
        normed = r.nrm[h]
        ng = normed_grad[:, 256 * h : 256 * h + 256]
        g = r.inv[h] * (ng - normed * jnp.mean(ng * normed, axis=1, keepdims=True))
        grads.append(g.astype(BF))
        inner = dotb(r.qr[h] * r.phd[h], grads[h], 0, 0)
        r.sa[1, pl.ds(4 * h, 4)] = inner.astype(BF).reshape(4, 32, VD)
    stage_a(1)
    give(3, far)

    query_parts, key_parts, value_parts = [], [], []
    for h in range(2):
        q, k, v, g = r.qr[h], r.kr[h], r.vh[h], grads[h]
        score = (dot(g, v, 1, 1) * r.mask[h]).astype(BF)
        query_parts.append(dotb(score, k, 1, 0) + r.phd[h] * dot(g, state_of(0, h), 1, 1))
        key_parts.append(dotb(score, q, 0, 0))
        value_parts.append(dot(r.wt[h], g, 0, 0))

    def together(parts):
        return dot(split, jnp.concatenate(parts, axis=0).astype(BF), 0, 0).astype(BF)

    r.o_query[...] = together([turn(p, cosines, -sines) for p in query_parts]).reshape(TOK, 2, KD)

    def project(*pieces):
        for i, _ in pieces:
            take(r.rt.at[pl.ds(0, 14)], r.q_recv.at[i])

        def rows_of(m):
            return jnp.concatenate(
                [r.rr[m, pl.ds(2 * q, 2)].reshape(64, TOK) for _, q in pieces], axis=0
            )

        part = dot(rows_of(0), r.na[0], 1, 0)
        for m in range(1, 8):
            part = part + dot(rows_of(m), r.na[m], 1, 0)
        for k, (_, q) in enumerate(pieces):
            r.zp[pl.ds(2 * q, 2)] = part[64 * k : 64 * k + 64].astype(BF).reshape(2, 32, 512)
            for to in (2 * q, 2 * q + 1):

                @pl.when(to != z)
                def _(to=to):
                    remote(r.zp.at[to], r.rz.at[z], r.p_send.at[1], r.p_recv, (to * 8 + j, x))

                @pl.when(to == z)
                def _():
                    r.rz[z] = r.zp[z]

    stage_b(1)
    take(r.nb, r.n_recv.at[0])
    take(r.na.at[pl.ds(0, 3)], r.n_recv.at[2])
    project((0, x), (1, left), (2, right), (3, far))
    stage_c(1)

    take(r.rz.at[pl.ds(0, 7)], r.p_recv)
    total = r.rz[0].astype(F32)
    for p in range(1, 8):
        total = total + r.rz[p].astype(F32)
    r.o_proj[...] = total

    take(r.rc.at[1, pl.ds(0, 7)], r.s_recv.at[1, 2])
    for h in range(2):
        future = state_of(1, h)
        key_parts[h] = key_parts[h] + r.rem[h] * dot(r.vh[h], future, 1, 1)
        value_parts[h] = value_parts[h] + r.rem[h] * dotb(r.kr[h], future, 1, 0)
    r.o_key[...] = together(
        [turn(p, cosines, -sines) * KD ** (-0.5) for p in key_parts]
    ).reshape(TOK, 2, KD)
    for i in range(2):
        at = slice(128 * i, 128 * i + 128)
        r.o_value[:, :, at] = together([p[:, at] for p in value_parts]).reshape(TOK, 2, 128)

    take(r.rg.at[pl.ds(0, 27)], r.d_send)
    take(r.rg.at[pl.ds(0, 36)], r.x_send)
    take(r.xin.at[:, pl.ds(0, 4)], r.r_send)
    take(r.fin.at[pl.ds(0, 63)], r.t_send)
    take(r.rt.at[pl.ds(0, 48)], r.g_send)
    for way in range(2):
        take(r.sa.at[way, pl.ds(0, 7)], r.s_send.at[way, 0])
        take(r.rb.at[way, pl.ds(0, 7)], r.s_send.at[way, 1])
        take(r.sc.at[way, pl.ds(0, 7)], r.s_send.at[way, 2])
    take(r.ta.at[pl.ds(0, 7)], r.u_send.at[0])
    take(r.tb.at[pl.ds(0, 7)], r.u_send.at[1])
    take(r.na.at[pl.ds(0, 7)], r.n_send)
    take(r.rr.at[pl.ds(0, 7)], r.p_send.at[0])
    take(r.zp.at[pl.ds(0, 7)], r.p_send.at[1])


def write_out(*refs):
    n = len(OUTPUTS)
    copies = [pltpu.make_async_copy(refs[i], refs[n + i], refs[2 * n].at[i]) for i in range(n)]
    for c in copies:
        c.start()
    for c in copies:
        c.wait()


def rotation_tables():
    frequency = np.repeat(10000.0 ** (-np.linspace(0.0, 1.0, KD // 2)), 2)[None, :]
    starts = np.arange(N_SP)[:, None] * TOK * frequency
    places = np.arange(TOK)[:, None] * frequency
    return tuple(
        np.concatenate([np.cos(a), np.sin(a)]).astype(np.float32) for a in (starts, places)
    )


def per_device(
    stream,
    out_grad,
    routes,
    route_weight,
    queries,
    key_vectors,
    value_vectors,
    log_decay,
    out_proj,
    gate_weight,
    up_weight,
    down_weight,
):
    starts, places = rotation_tables()
    anywhere = pl.BlockSpec(memory_space=pltpu.HBM)
    local = pl.BlockSpec(memory_space=pltpu.VMEM)
    results = pl.pallas_call(
        kernel,
        out_shape=tuple(pltpu.VMEM(*o) for o in OUTPUTS.values()),
        in_specs=(anywhere,) * len(INPUTS),
        out_specs=(local,) * len(OUTPUTS),
        scratch_shapes=[
            *(pltpu.VMEM(*b) for b in BUFFERS.values()),
            *(pltpu.SemaphoreType.DMA(s) if s else pltpu.SemaphoreType.DMA for s in SEMAPHORES.values()),
        ],
        compiler_params=pltpu.CompilerParams(
            collective_id=0, has_side_effects=True, vmem_limit_bytes=60 * 1024 * 1024
        ),
    )(
        stream,
        out_grad,
        routes.T,
        route_weight.T,
        queries,
        key_vectors,
        value_vectors,
        log_decay.T,
        out_proj,
        gate_weight,
        up_weight,
        down_weight,
        jnp.asarray(starts),
        jnp.asarray(places),
    )
    return pl.pallas_call(
        write_out,
        out_shape=tuple(jax.ShapeDtypeStruct(*o) for o in OUTPUTS.values()),
        in_specs=(local,) * len(OUTPUTS),
        out_specs=(anywhere,) * len(OUTPUTS),
        scratch_shapes=[pltpu.SemaphoreType.DMA((len(OUTPUTS),))],
        compiler_params=pltpu.CompilerParams(vmem_limit_bytes=1024 * 1024),
    )(*(pltpu.with_memory_space_constraint(a, pltpu.VMEM) for a in results))


def solution(mesh):
    by_position, by_head = P("sp", None), P("sp", "tp", None)
    columns, rows = P("sp", None, "tp"), P("sp", "tp", None)
    return jax.shard_map(
        per_device,
        mesh=mesh,
        in_specs=(
            *(by_position,) * 4,
            *(by_head,) * 3,
            P("sp", "tp"),
            P(None, "tp"),
            columns,
            columns,
            rows,
        ),
        out_specs=(columns, columns, rows, P("sp", "tp"), *(by_head,) * 3),
        check_vma=False,
    )
```

```python
import types

import jax
import jax.numpy as jnp
import numpy as np
from jax import lax
from jax.experimental import pallas as pl
from jax.experimental.pallas import tpu as pltpu
from jax.sharding import PartitionSpec as P

CLAMP_LIMIT = 7.0
GATE_SLOPE = 1.702
EPSILON = 1e-06
MESH = pl.DeviceIdType.MESH
BF = jnp.bfloat16
F32 = jnp.float32
HIGHEST = lax.Precision.HIGHEST

N_SP, N_TP = 64, 4
TOK, D, KD, VD = 128, 2048, 128, 256
QUART = D // N_TP
SHIFTS = (1, 7, 2, 6, 3, 5, 4)
WHOLE = (1, 7, 0)
BOTH = (1, 7)
PARTS = (1, 7, 2, 6, 3, 5, 4)
QUEUE = (
    (1, False),
    (7, False),
    (2, False),
    (6, False),
    (1, True),
    (7, True),
    (3, False),
    (5, False),
    (0, True),
    (4, False),
)
FIRST = 0
CHUNKS = (
    ((1, 0, 8), (7, 0, 8)),
    ((2, 0, 8), (6, 0, 8)),
    ((0, 0, 4), (0, 4, 4)),
    ((3, 0, 8), (5, 0, 8)),
    ((4, 0, 4), (4, 4, 4)),
)


def dot(a, b, ca, cb, precision=None):
    return lax.dot_general(
        a, b, (((ca,), (cb,)), ((), ())), preferred_element_type=F32, precision=precision
    )


def dotb(a, b, ca, cb):
    return dot(a.astype(BF), b.astype(BF), ca, cb)


def remote(src, dst, send_sem, recv_sem, device):
    pltpu.make_async_remote_copy(
        src_ref=src,
        dst_ref=dst,
        send_sem=send_sem,
        recv_sem=recv_sem,
        device_id=device,
        device_id_type=MESH,
    ).start()


def take(ref, sem):
    pltpu.make_async_copy(ref, ref, sem).wait()


def iota(shape, dim):
    return lax.broadcasted_iota(jnp.int32, shape, dim)


INPUTS = (
    "stream",
    "og",
    "in_routes",
    "in_weight",
    "in_queries",
    "in_keys",
    "in_values",
    "in_decay",
    "out_proj",
    "gate_w",
    "up_w",
    "down_w",
    "in_starts",
    "in_places",
)
SMALL = {
    "routes": ((2, TOK), jnp.int32),
    "weight": ((2, TOK), F32),
    "decay": ((2, TOK), F32),
    "starts": ((2 * N_SP, KD), F32),
    "places": ((2 * TOK, KD), F32),
    "queries": ((TOK, 2, KD), BF),
    "keys": ((TOK, 2, KD), BF),
    "values": ((TOK, 2, VD), BF),
}
OUTPUTS = {
    "o_gate": ((1, D, 256), BF),
    "o_up": ((1, D, 256), BF),
    "o_down": ((1, 256, D), BF),
    "o_proj": ((32, 512), F32),
    "o_query": ((TOK, 2, KD), BF),
    "o_key": ((TOK, 2, KD), BF),
    "o_value": ((TOK, 2, VD), BF),
}
LEFT = {
    **dict(list(OUTPUTS.items())[:5]),
    "kr": ((2, TOK, KD), F32),
    "vh": ((2, TOK, VD), BF),
    "rem": ((2, TOK, 1), F32),
    "kpart": ((2, TOK, KD), F32),
    "vpart": ((2, TOK, VD), F32),
    "future": ((2, KD, VD), BF),
    "turns": ((2, TOK, KD), F32),
}
BUFFERS = {
    **SMALL,
    "sf": ((TOK, D), BF),
    "of": ((TOK, D), BF),
    "ws": ((512, 1), F32),
    "w": ((D, 512), BF),
    "d": ((256, D), BF),
    "op": ((D, 512), BF),
    "pm": ((512, TOK), BF),
    "send": ((N_SP, 16, QUART), BF),
    "whole": ((3, 8, 4, 16, QUART), BF),
    "rg": ((N_SP, 4, 16, QUART), BF),
    "gu": ((512, 512), BF),
    "ac": ((512, 256), BF),
    "bk": ((4, N_SP, 8, QUART), BF),
    "xin": ((6, 5, 8, 8, QUART), BF),
    "acc": ((2, 5, 8, 8, QUART), BF),
    "fin": ((N_SP, 8, QUART), BF),
    "ret": ((N_SP, 8, QUART), BF),
    "rt": ((N_SP, 32, TOK), BF),
    "qr": ((2, TOK, KD), F32),
    "mask": ((2, TOK, TOK), F32),
    "wt": ((2, TOK, TOK), BF),
    "nrm": ((2, TOK, VD), F32),
    "inv": ((2, TOK, 1), F32),
    "phd": ((2, TOK, 1), F32),
    "sa": ((2, 8, 32, VD), BF),
    "ra": ((2, 8, 32, VD), BF),
    "pp": ((2, 8, 32, VD), F32),
    "sb": ((2, 32, VD), BF),
    "rb": ((2, 8, 32, VD), BF),
    "sc": ((2, 8, 32, VD), BF),
    "rc": ((2, 8, 32, VD), BF),
    "run": ((32, VD), F32),
    "tmine": ((2, VD), F32),
    "tplane": ((2, VD), F32),
    "ta": ((8, 2, VD), F32),
    "tb": ((8, 2, VD), F32),
    "nb": ((TOK, 512), BF),
    "na": ((8, TOK, 512), BF),
    "rr": ((8, 8, 32, TOK), BF),
    "zp": ((8, 32, 512), BF),
    "rz": ((8, 32, 512), BF),
}
SEMAPHORES = {
    "load": (14,),
    "d_send": (),
    "d_recv": (2, 8),
    "x_send": (),
    "x_recv": (4, 8),
    "r_send": (),
    "r_recv": (6, 5),
    "t_send": (),
    "t_recv": (),
    "g_send": (),
    "g_recv": (6,),
    "s_send": (2, 3),
    "s_recv": (2, 3),
    "b_send": (2, 8),
    "b_recv": (2, 8),
    "u_send": (2,),
    "u_recv": (2,),
    "n_send": (),
    "n_recv": (3,),
    "p_send": (2,),
    "p_recv": (),
    "q_recv": (4,),
}
NAMES = (*INPUTS, *LEFT, *BUFFERS, *SEMAPHORES)


def turn(field, cosines, sines):
    odd = iota((TOK, KD), 1) % 2 == 1
    partner = jnp.where(odd, pltpu.roll(field, 1, 1), pltpu.roll(field, KD - 1, 1))
    return field * cosines + partner * sines


def apart():
    a, b = iota((256, 256), 0), iota((256, 256), 1)
    return (b == 2 * (a % 128) + a // 128).astype(BF)


def together(parts):
    return dot(apart(), jnp.concatenate(parts, axis=0).astype(BF), 0, 0).astype(BF)


def kernel(*refs):
    r = types.SimpleNamespace(**dict(zip(NAMES, refs, strict=True)))
    me = lax.axis_index("sp")
    x = lax.axis_index("tp")
    z, j = me // 8, me % 8
    other = j + 1 - 2 * (j % 2)
    right, left, far = (x + 1) % 4, (x + 3) % 4, (x + 2) % 4

    def plane(dz):
        return (z + dz) % 8

    cols = pl.ds(pl.multiple_of(x * QUART, QUART), QUART)
    barrier = pltpu.get_barrier_semaphore()

    def hello(k, _):
        pl.semaphore_signal(barrier, inc=1, device_id=((me + k) % 64, x), device_id_type=MESH)
        return 0

    lax.fori_loop(32, 64, hello, 0)
    lax.fori_loop(1, 32, hello, 0)
    for peer in (right, left, far):
        pl.semaphore_signal(barrier, inc=1, device_id=(me, peer), device_id_type=MESH)

    copies = [
        (r.in_routes, r.routes),
        (r.in_weight, r.weight),
        (r.stream, r.sf),
        (r.og, r.of),
        *((getattr(r, "in_" + name), getattr(r, name)) for name in list(SMALL)[2:]),
        (r.gate_w.at[0], r.w.at[:, pl.ds(0, 256)]),
        (r.up_w.at[0], r.w.at[:, pl.ds(256, 256)]),
        (r.down_w.at[0], r.d),
        (r.out_proj, r.op),
    ]
    loads = [pltpu.make_async_copy(*c, r.load.at[i]) for i, c in enumerate(copies)]
    for c in loads:
        c.start()

    rows, lanes = iota((TOK, TOK), 0), iota((TOK, TOK), 1)
    loads[0].wait()
    loads[1].wait()
    ids = r.routes[...].astype(F32)
    wrow = r.weight[...]
    expert = iota((64, TOK), 0).astype(F32)
    named0 = (expert == ids[0:1]).astype(F32)
    named1 = (expert == ids[1:2]).astype(F32)
    before = dotb(named0 + named1, (rows < lanes).astype(F32), 1, 0)
    dest0 = ids[0:1] * 8.0 + jnp.sum(named0 * before, axis=0, keepdims=True)
    dest1 = ids[1:2] * 8.0 + jnp.sum(named1 * before, axis=0, keepdims=True)
    slot = iota((512, TOK), 0).astype(F32)
    at0 = (slot == dest0).astype(F32)
    at1 = (slot == dest1).astype(F32)
    wslot = jnp.sum(at0 * wrow[0:1] + at1 * wrow[1:2], axis=1, keepdims=True)
    place = (at0 + at1).astype(BF)
    r.pm[...] = place
    r.ws[...] = wslot
    loads[2].wait()
    r.send[:, 0:8, :] = dot(place, r.sf[:, cols], 1, 0).reshape(64, 8, QUART).astype(BF)
    loads[3].wait()
    r.send[:, 8:16, :] = (dot(place, r.of[:, cols], 1, 0) * wslot).reshape(64, 8, QUART).astype(BF)

    pl.semaphore_wait(barrier, 66)

    mine, others = j // 4 * 4, 4 - j // 4 * 4

    def dispatch(dz, whole):
        def send_to(m):
            p = plane(dz) * 8 + m
            if whole:
                block, slot_of = r.whole.at[WHOLE.index(dz), m], r.rg.at[me]
            else:
                block, slot_of = r.send.at[p], r.rg.at[me, x]
            remote(block, slot_of, r.d_send, r.d_recv.at[int(whole), dz], (p, x))

        def one(k, _):
            send_to((j + k) % 8)
            return 0

        def one_of_half(k, _):
            send_to((mine if whole else others) + (j + k) % 4)
            return 0

        if dz in BOTH:
            lax.fori_loop(0, 4, one_of_half, 0)
        else:
            lax.fori_loop(1 if dz == 0 else 0, 8, one, 0)

    def build_whole():
        for i, dz in enumerate(WHOLE):
            at = pl.ds(pl.multiple_of(plane(dz) * 64, 64), 64)
            slots, scale = r.pm[at, :], r.ws[at, :]
            for q in range(4):
                these = slice(q * QUART, (q + 1) * QUART)
                rows_q = dot(slots, r.sf[:, these], 1, 0)
                grads_q = dot(slots, r.of[:, these], 1, 0) * scale
                r.whole[i, :, q, 0:8, :] = rows_q.reshape(8, 8, QUART).astype(BF)
                r.whole[i, :, q, 8:16, :] = grads_q.reshape(8, 8, QUART).astype(BF)

    first_whole = [whole for _, whole in QUEUE].index(True)
    for at, (dz, whole) in enumerate(QUEUE):
        if at == first_whole:
            build_whole()
        dispatch(dz, whole)
    r.rg[me] = r.whole[WHOLE.index(0), j]

    odd = lanes % 2 == 1

    def angles():
        ca, sa = r.starts[pl.ds(me, 1), :], r.starts[pl.ds(me + 64, 1), :]
        cb, sb = r.places[0:128, :], r.places[128:256, :]
        return ca * cb - sa * sb, jnp.where(odd, 1.0, -1.0) * (sa * cb + ca * sb)

    for c in loads[4:10]:
        c.wait()
    cosines, sines = angles()
    r.turns[0], r.turns[1] = cosines, sines
    split = apart()
    q2 = dot(split, r.queries[...].reshape(256, KD), 1, 0)
    k2 = dot(split, r.keys[...].reshape(256, KD), 1, 0)
    v2 = [dot(split, r.values[:, :, 128 * i : 128 * i + 128].reshape(256, 128), 1, 0) for i in (0, 1)]
    decay = r.decay[...]
    cum_row = dot(decay, (rows <= lanes).astype(F32), 1, 0, HIGHEST)
    cum_col = dot((rows >= lanes).astype(F32), decay, 1, 1, HIGHEST)
    causal = rows >= lanes
    for h in range(2):
        at = slice(128 * h, 128 * h + 128)
        q = turn(q2[at], cosines, sines)
        k = turn(k2[at], cosines, sines) * KD ** (-0.5)
        r.qr[h] = q
        r.kr[h] = k
        r.vh[h, :, 0:128] = v2[0][at].astype(BF)
        r.vh[h, :, 128:256] = v2[1][at].astype(BF)
        col = cum_col[:, h : h + 1]
        total = cum_col[127:128, h : h + 1]
        rem = jnp.exp(total - col)
        r.phd[h] = jnp.exp(col)
        r.rem[h] = rem
        diff = col - cum_row[h : h + 1, :]
        mask = jnp.where(causal, jnp.exp(jnp.where(causal, diff, 0.0)), 0.0)
        r.mask[h] = mask
        state = dotb(k * rem, r.vh[h], 0, 0)
        r.sa[0, pl.ds(4 * h, 4)] = state.astype(BF).reshape(4, 32, VD)
        r.tmine[h : h + 1, :] = jnp.broadcast_to(total, (1, VD))

    def within(src, dst, send_sem, recv_sem):
        def one(k, _):
            m = (j + k) % 8
            remote(src(m), dst(j), send_sem, recv_sem, (z * 8 + m, x))
            return 0

        lax.fori_loop(1, 8, one, 0)

    def over_z(src, dst, send_sem, recv_sem):
        for dz in PARTS:
            remote(src(plane(dz)), dst(z), send_sem, recv_sem, (plane(dz) * 8 + j, x))

    def stage_a(way):
        within(
            lambda m: r.sa.at[way, m],
            lambda m: r.ra.at[way, m],
            r.s_send.at[way, 0],
            r.s_recv.at[way, 0],
        )
        r.ra[way, j] = r.sa[way, j]
        if way == 0:
            within(lambda m: r.tmine, lambda m: r.ta.at[m], r.u_send.at[0], r.u_recv.at[0])
            r.ta[j] = r.tmine[...]

    head = pl.ds(j // 4, 1)

    def stage_b(way):
        take(r.ra.at[way, pl.ds(0, 7)], r.s_recv.at[way, 0])
        if way == 0:
            take(r.ta.at[pl.ds(0, 7)], r.u_recv.at[0])
            total = r.ta[0]
            for m in range(1, 8):
                total = total + r.ta[m]
            r.tplane[...] = total
        run = jnp.zeros((32, VD), F32)
        for m in range(8) if way == 0 else reversed(range(8)):
            r.pp[way, m] = run
            run = jnp.exp(r.ta[m, head, :]) * run + r.ra[way, m].astype(F32)
        r.sb[way] = run.astype(BF)
        for dz in PARTS:
            p = plane(dz)

            @pl.when((p > z) if way == 0 else (p < z))
            def _(p=p):
                remote(
                    r.sb.at[way],
                    r.rb.at[way, z],
                    r.b_send.at[way, p],
                    r.b_recv.at[way, z],
                    (p * 8 + j, x),
                )

        if way == 0:
            over_z(lambda p: r.tplane, lambda p: r.tb.at[p], r.u_send.at[1], r.u_recv.at[1])
            r.tb[z] = r.tplane[...]

    def stage_c(way):
        if way == 0:
            take(r.tb.at[pl.ds(0, 7)], r.u_recv.at[1])
        r.run[...] = jnp.zeros((32, VD), F32)
        for p in range(8) if way == 0 else reversed(range(8)):

            @pl.when((p < z) if way == 0 else (p > z))
            def _(p=p):
                take(r.rb.at[way, p], r.b_recv.at[way, p])
                r.run[...] = jnp.exp(r.tb[p, head, :]) * r.run[...] + r.rb[way, p].astype(F32)

        run = r.run[...]
        logs = jnp.zeros((1, VD), F32)
        for m in range(8) if way == 0 else reversed(range(8)):
            r.sc[way, m] = (jnp.exp(logs) * run + r.pp[way, m]).astype(BF)
            logs = logs + r.ta[m, head, :]
        within(
            lambda m: r.sc.at[way, m],
            lambda m: r.rc.at[way, m],
            r.s_send.at[way, 2],
            r.s_recv.at[way, 2],
        )
        r.rc[way, j] = r.sc[way, j]

    def state_of(way, h):
        return r.rc[way, pl.ds(4 * h, 4)].reshape(128, VD)

    def normalise():
        take(r.rc.at[0, pl.ds(0, 7)], r.s_recv.at[0, 2])
        for h in range(2):
            q, k, v = r.qr[h], r.kr[h], r.vh[h]
            weights = (dotb(q, k, 1, 1) * r.mask[h]).astype(BF)
            r.wt[h] = weights
            kept = dot(weights, v, 1, 0) + r.phd[h] * dotb(q, state_of(0, h), 1, 0)
            inv = lax.rsqrt(jnp.mean(kept * kept, axis=1, keepdims=True) + EPSILON)
            r.inv[h] = inv
            r.nrm[h] = kept * inv
            r.nb[:, 256 * h : 256 * h + 256] = (kept * inv).astype(BF)
        r.na[j] = r.nb[...]

    def share_normed():
        remote(r.nb, r.na.at[j], r.n_send, r.n_recv.at[0], (z * 8 + other, x))
        for k in range(1, 4):
            m = (j + 2 * k) % 8
            remote(r.nb, r.na.at[j], r.n_send, r.n_recv.at[1], (z * 8 + m, x))

    def relay():
        take(r.na.at[pl.ds(0, 3)], r.n_recv.at[1])
        for k in range(1, 4):
            m = (j + 2 * k) % 8
            remote(r.na.at[m], r.na.at[m], r.n_send, r.n_recv.at[2], (z * 8 + other, x))

    def senders(dz):
        if dz in BOTH:
            return plane(8 - dz) * 8 + others, 4
        return plane(8 - dz) * 8, 8

    def group(q, dz):
        first, n = senders(dz)
        return r.rg.at[pl.ds(first, n), q]

    def half(q, dz, h):
        first, n = senders(dz)
        return r.rg.at[pl.ds(first + h * (n // 2), n // 2), q]

    def spread(dz):
        take(group(x, dz), r.d_recv.at[0, dz])
        remote(group(x, dz), group(x, dz), r.x_send, r.x_recv.at[0, dz], (me, right))
        remote(group(x, dz), group(x, dz), r.x_send, r.x_recv.at[1, dz], (me, left))

    def pass_on(dz):
        take(group(left, dz), r.x_recv.at[0, dz])
        remote(half(left, dz, 0), half(left, dz, 0), r.x_send, r.x_recv.at[2, dz], (me, right))
        take(group(right, dz), r.x_recv.at[1, dz])
        remote(half(right, dz, 1), half(right, dz, 1), r.x_send, r.x_recv.at[3, dz], (me, left))

    def complete(dz):
        if dz in PARTS:
            take(half(far, dz, 0), r.x_recv.at[2, dz])
            take(half(far, dz, 1), r.x_recv.at[3, dz])
        if dz in BOTH:
            take(r.rg.at[pl.ds(plane(8 - dz) * 8 + mine, 4)], r.d_recv.at[1, dz])
        elif dz in WHOLE:
            take(r.rg.at[pl.ds(0, 7)], r.d_recv.at[1, dz])

    def block(m, part):
        dz, first, n = CHUNKS[m][part]
        return plane(8 - dz) * 8 + first, n

    def experts(m):
        for dz in dict.fromkeys(c[0] for c in CHUNKS[m]):
            complete(dz)
        if m == FIRST:
            for c in loads[10:]:
                c.wait()
        (fa, na), (fb, nb) = block(m, 0), block(m, 1)

        def both(q, part):
            these = pl.ds(8 * part, 8)
            a = r.rg[pl.ds(fa, na), q, these, :].reshape(8 * na, QUART)
            b = r.rg[pl.ds(fb, nb), q, these, :].reshape(8 * nb, QUART)
            return jnp.concatenate([a, b], axis=0)

        pre = dot(both(0, 0), r.w[0:QUART, :], 1, 0)
        back = dot(both(0, 1), r.d[:, 0:QUART], 1, 1)
        for q in range(1, 4):
            pre = pre + dot(both(q, 0), r.w[q * QUART : (q + 1) * QUART, :], 1, 0)
            back = back + dot(both(q, 1), r.d[:, q * QUART : (q + 1) * QUART], 1, 1)
        gate_pre, up_pre = pre[:, 0:256], pre[:, 256:512]
        gate_clip = jnp.minimum(gate_pre, CLAMP_LIMIT)
        up_clip = jnp.clip(up_pre, -CLAMP_LIMIT, CLAMP_LIMIT)
        sig = jax.nn.sigmoid(GATE_SLOPE * gate_clip)
        activated = (gate_clip * sig * (up_clip + 1.0)).astype(BF)
        slope = sig + GATE_SLOPE * gate_clip * sig * (1.0 - sig)
        gate_g = jnp.where(gate_pre < CLAMP_LIMIT, back * (up_clip + 1.0) * slope, 0.0).astype(BF)
        up_g = jnp.where(jnp.abs(up_pre) < CLAMP_LIMIT, back * gate_clip * sig, 0.0).astype(BF)
        both_g = jnp.concatenate([gate_g, up_g], axis=1)
        for lo, first, n in ((0, fa, na), (8 * na, fb, nb)):
            at = pl.ds(pl.multiple_of(first * 8, 32), 8 * n)
            r.gu[at, :] = both_g[lo : lo + 8 * n]
            r.ac[at, :] = activated[lo : lo + 8 * n]
        for q in range(4):
            out = dot(both_g, r.w[q * QUART : (q + 1) * QUART, :], 1, 1).astype(BF)
            for lo, first, n in ((0, fa, na), (8 * na, fb, nb)):
                r.bk[q, pl.ds(first, n)] = out[lo : lo + 8 * n].reshape(n, 8, QUART)

        pa, pb = pl.ds(fa, na), pl.ds(fb, nb)
        for k, rows_of, to in (
            (0, r.bk.at[far, pa], right),
            (1, r.bk.at[far, pb], left),
            (2, r.bk.at[left, pa], left),
            (3, r.bk.at[right, pb], right),
        ):
            space = r.xin.at[k, m, pl.ds(0, nb if k % 2 else na)]
            remote(rows_of, space, r.r_send, r.r_recv.at[k, m], (me, to))

    def forward(m):
        for part, mine_of, to in ((0, right, right), (1, left, left)):
            first, n = block(m, part)
            at, here = pl.ds(0, n), pl.ds(first, n)
            take(r.xin.at[part, m, at], r.r_recv.at[part, m])
            r.acc[part, m, at] = (
                r.xin[part, m, at].astype(F32) + r.bk[mine_of, here].astype(F32)
            ).astype(BF)
            remote(
                r.acc.at[part, m, at],
                r.xin.at[4 + part, m, at],
                r.r_send,
                r.r_recv.at[4 + part, m],
                (me, to),
            )

    def finish(m):
        for part in range(2):
            dz = CHUNKS[m][part][0]
            first, n = block(m, part)
            at, here = pl.ds(0, n), pl.ds(first, n)
            direct, summed = 2 + part, 4 + part
            take(r.xin.at[direct, m, at], r.r_recv.at[direct, m])
            take(r.xin.at[summed, m, at], r.r_recv.at[summed, m])
            r.fin[here] = (
                r.bk[x, here].astype(F32)
                + r.xin[direct, m, at].astype(F32)
                + r.xin[summed, m, at].astype(F32)
            ).astype(BF)

            def one(k, _, first=first, n=n, dz=dz):
                p = first + (j + k) % n
                if dz == 0:

                    @pl.when(p != me)
                    def _():
                        remote(r.fin.at[p], r.ret.at[me], r.t_send, r.t_recv, (p, x))

                else:
                    remote(r.fin.at[p], r.ret.at[me], r.t_send, r.t_recv, (p, x))
                return 0

            lax.fori_loop(0, n, one, 0)
            if dz == 0:

                @pl.when((me >= first) & (me < first + n))
                def _():
                    r.ret[me] = r.fin[me]

    def weight_grads(q):
        at = pl.ds(q * QUART, QUART)
        rows_q = r.rg[:, q, 0:8, :].reshape(512, QUART)
        grads_q = r.rg[:, q, 8:16, :].reshape(512, QUART)
        both = dot(rows_q, r.gu[...], 0, 0).astype(BF)
        r.o_gate[0, at, :] = both[:, 0:256]
        r.o_up[0, at, :] = both[:, 256:512]
        r.o_down[0, :, at] = dot(r.ac[...], grads_q, 0, 0).astype(BF)

    spread(1)
    spread(7)
    stage_a(0)
    pass_on(1)
    pass_on(7)
    spread(2)
    spread(6)
    pass_on(2)
    pass_on(6)
    experts(0)
    spread(3)
    forward(0)
    spread(5)
    pass_on(3)
    experts(1)
    pass_on(5)
    finish(0)
    spread(4)
    forward(1)
    stage_b(0)
    experts(2)
    experts(3)
    pass_on(4)
    finish(1)
    stage_c(0)
    forward(2)
    forward(3)
    experts(4)
    finish(2)
    normalise()
    finish(3)
    weight_grads(0)
    forward(4)
    weight_grads(1)
    finish(4)
    share_normed()
    weight_grads(2)
    weight_grads(3)

    def quarter(q):
        return pl.ds(q * 16, 16)

    take(r.ret.at[pl.ds(0, 63)], r.t_recv)
    same = (rows == lanes).astype(BF)
    resid = dot(r.ret[...].reshape(512, QUART), r.pm[...], 0, 0) + dot(r.of[:, cols], same, 0, 0)
    r.rt[quarter(x)] = resid.astype(BF).reshape(16, 32, TOK)
    def part_of(q, h):
        return r.rt.at[pl.ds(q * 16 + 8 * h, 8)]

    for k, (h, peer) in enumerate(((0, right), (1, left), (1, right), (0, left))):
        remote(part_of(x, h), part_of(x, h), r.g_send, r.g_recv.at[k], (me, peer))

    def give(i, q):
        def one(k, _):
            m = (j + k) % 8
            for p in (2 * q, 2 * q + 1):
                remote(
                    r.rt.at[p * 8 + m],
                    r.rr.at[j, p],
                    r.p_send.at[0],
                    r.q_recv.at[i],
                    (z * 8 + m, x),
                )
            return 0

        lax.fori_loop(1, 8, one, 0)
        for p in (2 * q, 2 * q + 1):
            r.rr[j, p] = r.rt[p * 8 + j]

    give(0, x)

    def share(q):
        rows_q = pl.ds(pl.multiple_of(q * QUART, QUART), QUART)
        return dot(r.rt[quarter(q)].reshape(QUART, TOK), r.op[rows_q, :], 0, 0)

    take(part_of(left, 0), r.g_recv.at[0])
    remote(part_of(left, 0), part_of(left, 0), r.g_send, r.g_recv.at[4], (me, right))
    take(part_of(right, 1), r.g_recv.at[1])
    remote(part_of(right, 1), part_of(right, 1), r.g_send, r.g_recv.at[5], (me, left))
    take(part_of(left, 1), r.g_recv.at[2])
    take(part_of(right, 0), r.g_recv.at[3])
    relay()
    give(1, left)
    give(2, right)
    normed_grad = share(x) + share(left) + share(right)
    take(part_of(far, 0), r.g_recv.at[4])
    take(part_of(far, 1), r.g_recv.at[5])
    normed_grad = normed_grad + share(far)

    def project(*pieces):
        for i, _ in pieces:
            take(r.rt.at[pl.ds(0, 14)], r.q_recv.at[i])

        def rows_of(m):
            return jnp.concatenate(
                [r.rr[m, pl.ds(2 * q, 2)].reshape(64, TOK) for _, q in pieces], axis=0
            )

        part = dot(rows_of(0), r.na[0], 1, 0)
        for m in range(1, 8):
            part = part + dot(rows_of(m), r.na[m], 1, 0)
        for k, (_, q) in enumerate(pieces):
            r.zp[pl.ds(2 * q, 2)] = part[64 * k : 64 * k + 64].astype(BF).reshape(2, 32, 512)
            for to in (2 * q, 2 * q + 1):

                @pl.when(to != z)
                def _(to=to):
                    remote(r.zp.at[to], r.rz.at[z], r.p_send.at[1], r.p_recv, (to * 8 + j, x))

                @pl.when(to == z)
                def _():
                    r.rz[z] = r.zp[z]

    grads = []
    for h in range(2):
        normed = r.nrm[h]
        ng = normed_grad[:, 256 * h : 256 * h + 256]
        g = r.inv[h] * (ng - normed * jnp.mean(ng * normed, axis=1, keepdims=True))
        grads.append(g.astype(BF))
        inner = dotb(r.qr[h] * r.phd[h], grads[h], 0, 0)
        r.sa[1, pl.ds(4 * h, 4)] = inner.astype(BF).reshape(4, 32, VD)
    stage_a(1)
    give(3, far)
    take(r.nb, r.n_recv.at[0])
    take(r.na.at[pl.ds(0, 3)], r.n_recv.at[2])
    project((0, x))

    query_parts = []
    for h in range(2):
        q, k, v, g = r.qr[h], r.kr[h], r.vh[h], grads[h]
        score = (dot(g, v, 1, 1) * r.mask[h]).astype(BF)
        query_parts.append(dotb(score, k, 1, 0) + r.phd[h] * dot(g, state_of(0, h), 1, 1))
        r.kpart[h] = dotb(score, q, 0, 0)
        r.vpart[h] = dot(r.wt[h], g, 0, 0)

    r.o_query[...] = together([turn(p, cosines, -sines) for p in query_parts]).reshape(TOK, 2, KD)

    stage_b(1)
    project((1, left), (2, right), (3, far))
    stage_c(1)

    take(r.rz.at[pl.ds(0, 7)], r.p_recv)
    total = r.rz[0].astype(F32)
    for p in range(1, 8):
        total = total + r.rz[p].astype(F32)
    r.o_proj[...] = total

    take(r.rc.at[1, pl.ds(0, 7)], r.s_recv.at[1, 2])
    for h in range(2):
        r.future[h] = state_of(1, h)

    take(r.rg.at[pl.ds(0, 27)], r.d_send)
    take(r.rg.at[pl.ds(0, 36)], r.x_send)
    take(r.xin.at[:, pl.ds(0, 4)], r.r_send)
    take(r.fin.at[pl.ds(0, 63)], r.t_send)
    take(r.rt.at[pl.ds(0, 48)], r.g_send)
    for way in range(2):
        take(r.sa.at[way, pl.ds(0, 7)], r.s_send.at[way, 0])
        for p in range(8):

            @pl.when((p > z) if way == 0 else (p < z))
            def _(p=p):
                take(r.sb.at[way], r.b_send.at[way, p])

        take(r.sc.at[way, pl.ds(0, 7)], r.s_send.at[way, 2])
    take(r.ta.at[pl.ds(0, 7)], r.u_send.at[0])
    take(r.tb.at[pl.ds(0, 7)], r.u_send.at[1])
    take(r.na.at[pl.ds(0, 7)], r.n_send)
    take(r.rr.at[pl.ds(0, 7)], r.p_send.at[0])
    take(r.zp.at[pl.ds(0, 7)], r.p_send.at[1])


def last_step(*refs):
    n, m = len(LEFT), len(OUTPUTS)
    r = types.SimpleNamespace(**dict(zip(LEFT, refs[:n], strict=True)))
    outs, (key, value, sems) = refs[n : n + m], refs[n + m :]
    ready = [*refs[:5], key, value]
    copies = [pltpu.make_async_copy(ready[i], outs[i], sems.at[i]) for i in range(m)]
    for c in copies[:5]:
        c.start()
    cosines, sines = r.turns[0], r.turns[1]
    keys, values = [], []
    for h in range(2):
        k = r.kpart[h] + r.rem[h] * dot(r.vh[h], r.future[h], 1, 1)
        keys.append(turn(k, cosines, -sines) * KD ** (-0.5))
        values.append(r.vpart[h] + r.rem[h] * dotb(r.kr[h], r.future[h], 1, 0))
    key[...] = together(keys).reshape(TOK, 2, KD)
    copies[5].start()
    for i in range(2):
        at = slice(128 * i, 128 * i + 128)
        value[:, :, at] = together([v[:, at] for v in values]).reshape(TOK, 2, 128)
    copies[6].start()
    for c in copies:
        c.wait()


def rotation_tables():
    frequency = np.repeat(10000.0 ** (-np.linspace(0.0, 1.0, KD // 2)), 2)[None, :]
    starts = np.arange(N_SP)[:, None] * TOK * frequency
    places = np.arange(TOK)[:, None] * frequency
    return tuple(
        np.concatenate([np.cos(a), np.sin(a)]).astype(np.float32) for a in (starts, places)
    )


def per_device(
    stream,
    out_grad,
    routes,
    route_weight,
    queries,
    key_vectors,
    value_vectors,
    log_decay,
    out_proj,
    gate_weight,
    up_weight,
    down_weight,
):
    starts, places = rotation_tables()
    anywhere = pl.BlockSpec(memory_space=pltpu.HBM)
    local = pl.BlockSpec(memory_space=pltpu.VMEM)
    results = pl.pallas_call(
        kernel,
        out_shape=tuple(pltpu.VMEM(*o) for o in LEFT.values()),
        in_specs=(anywhere,) * len(INPUTS),
        out_specs=(local,) * len(LEFT),
        scratch_shapes=[
            *(pltpu.VMEM(*b) for b in BUFFERS.values()),
            *(pltpu.SemaphoreType.DMA(s) if s else pltpu.SemaphoreType.DMA for s in SEMAPHORES.values()),
        ],
        compiler_params=pltpu.CompilerParams(
            collective_id=0, has_side_effects=True, vmem_limit_bytes=62_600_000
        ),
    )(
        stream,
        out_grad,
        routes.T,
        route_weight.T,
        queries,
        key_vectors,
        value_vectors,
        log_decay.T,
        out_proj,
        gate_weight,
        up_weight,
        down_weight,
        jnp.asarray(starts),
        jnp.asarray(places),
    )
    return pl.pallas_call(
        last_step,
        out_shape=tuple(jax.ShapeDtypeStruct(*o) for o in OUTPUTS.values()),
        in_specs=(local,) * len(LEFT),
        out_specs=(anywhere,) * len(OUTPUTS),
        scratch_shapes=[
            pltpu.VMEM((TOK, 2, KD), BF),
            pltpu.VMEM((TOK, 2, VD), BF),
            pltpu.SemaphoreType.DMA((len(OUTPUTS),)),
        ],
        compiler_params=pltpu.CompilerParams(vmem_limit_bytes=8 * 1024 * 1024),
    )(*(pltpu.with_memory_space_constraint(a, pltpu.VMEM) for a in results))


def solution(mesh):
    by_position, by_head = P("sp", None), P("sp", "tp", None)
    columns, rows = P("sp", None, "tp"), P("sp", "tp", None)
    return jax.shard_map(
        per_device,
        mesh=mesh,
        in_specs=(
            *(by_position,) * 4,
            *(by_head,) * 3,
            P("sp", "tp"),
            P(None, "tp"),
            columns,
            columns,
            rows,
        ),
        out_specs=(columns, columns, rows, P("sp", "tp"), *(by_head,) * 3),
        check_vma=False,
    )
```
